32 devices in a mesh: sp: 8 (over z, y), tp: 4 (over x, core).
Axes of the slice: x: 2, y: 2, z: 4, core: 2. Of those that a mesh axis runs over, the one named last changes fastest.
Arguments:
- residual: bfloat16 [5120, 2048], P('sp', 'tp'), may hold values from -4 to 4
- query_wide: bfloat16 [5120, 1536], P('sp', 'tp'), may hold values from -500 to 500
- query_narrow: bfloat16 [5120, 1024], P('sp', 'tp'), may hold values from -500 to 500
- latent: bfloat16 [5120, 512], P('sp'), may hold values from -6 to 6
- rope_key: bfloat16 [5120, 64], P('sp'), may hold values from -6 to 6
- latent_gain: float32 [512], replicated, may hold values from 0.1 to 1.9
- expand_wide: bfloat16 [512, 2048], P(None, 'tp'), may hold values from -0.25 to 0.25
- expand_narrow: bfloat16 [512, 1024], P(None, 'tp'), may hold values from -0.25 to 0.25
- out_wide: bfloat16 [1024, 2048], P('tp'), may hold values from -0.1875 to 0.1875
- out_narrow: bfloat16 [512, 2048], P('tp'), may hold values from -0.25 to 0.25
- norm_gain: float32 [2048], P('tp'), may hold values from 0.1 to 1.9
- up_gate: bfloat16 [2048, 5632], P('sp', 'tp'), may hold values from -0.125 to 0.125
- up_value: bfloat16 [2048, 5632], P('sp', 'tp'), may hold values from -0.125 to 0.125
- down_weight: bfloat16 [2048, 5632], P('sp', 'tp'), may hold values from -0.078125 to 0.078125
- conv_taps: float32 [3, 2, 5632], P(None, None, 'tp'), may hold values from -3 to 3
Outputs:
- output: bfloat16 [5120, 2048], P('sp', 'tp')
The draws below stay inside these ranges and needn't reach their ends.
All inputs are finite; a program needn't handle non-finite values.
Results may differ from the reference program's by a relative error of at most 0.025.
Values may be sent and summed in bfloat16 or wider, within the bound.
A program may use at most 192 MiB of HBM per device.

```python
import math
import jax
import jax.numpy as jnp
from jax import lax

D = 2048
FF = 5632
RANK = 512
ROPE = 64
HW = 8
NOPE_W = 128
VAL_W = 128
HN = 8
NOPE_N = 64
VAL_N = 64
TOKENS = 5120
N_TP = 4


def draw_residual(key, part):
    key_noise = jax.random.fold_in(key, 11)
    columns = jnp.arange(D, dtype=jnp.float32) / D
    values = jax.random.normal(key_noise, (TOKENS, D), jnp.float32) * 0.1 * jnp.exp(1.6 * columns)[None, :]
    return jnp.clip(values, -4.0, 4.0).astype(jnp.bfloat16)


def query_values(key, arr_shape):
    key_noise = jax.random.fold_in(key, 21)
    values = jax.random.normal(key_noise, arr_shape, jnp.float32) * 2.5
    return jnp.clip(values, -12.0, 12.0)


def draw_query_wide(key, part):
    return query_values(jax.random.fold_in(key, 1), (TOKENS, HW * (NOPE_W + ROPE))).astype(jnp.bfloat16)


def draw_query_narrow(key, part):
    return query_values(jax.random.fold_in(key, 2), (TOKENS, HN * (NOPE_N + ROPE))).astype(jnp.bfloat16)


def level_of(key, dims, cuts, smallest, high):
    gain = 1.0
    for dim, blocks in cuts:
        draws = jax.random.uniform(jax.random.fold_in(jax.random.fold_in(key, 6), dim), (blocks,), jnp.float32, smallest / len(cuts), high / len(cuts))
        gain = gain * jnp.repeat(jnp.exp(draws), dims[dim] // blocks).reshape((-1,) + (1,) * (len(dims) - 1 - dim))
    return gain


def scatter_about(key, extent, scale, reach, cuts=(), kind=jnp.bfloat16):
    level = level_of(key, extent, cuts, -0.22, 0.18) if cuts else 1.0
    values = jax.random.normal(key, extent, jnp.float32) * scale * level
    return jnp.minimum(jnp.maximum(values, -reach), reach).astype(kind)


def setup_inputs(seed: int = 0) -> dict:
    arg_keys = jax.random.split(jax.random.key(seed), 16)
    return {
        "residual": draw_residual(jax.random.fold_in(arg_keys[15], 71), 0),
        "query_wide": draw_query_wide(jax.random.fold_in(arg_keys[15], 71), 0),
        "query_narrow": draw_query_narrow(jax.random.fold_in(arg_keys[15], 71), 0),
        "latent": scatter_about(arg_keys[3], (TOKENS, RANK), 1.0, 6.0, ((0, 8),)),
        "rope_key": scatter_about(arg_keys[4], (TOKENS, ROPE), 1.0, 6.0, ((0, 8),)),
        "latent_gain": jnp.clip(1.0 + 0.18 * jax.random.normal(arg_keys[5], (RANK,), jnp.float32), 0.1, 1.9),
        "expand_wide": scatter_about(arg_keys[6], (RANK, HW * (NOPE_W + VAL_W)), RANK ** -0.5, 0.25, ((1, 4),)),
        "expand_narrow": scatter_about(arg_keys[7], (RANK, HN * (NOPE_N + VAL_N)), RANK ** -0.5, 0.25, ((1, 4),)),
        "out_wide": scatter_about(arg_keys[8], (HW * VAL_W, D), (HW * VAL_W) ** -0.5, 0.1875, ((0, 4),)),
        "out_narrow": scatter_about(arg_keys[9], (HN * VAL_N, D), (HN * VAL_N) ** -0.5, 0.25, ((0, 4),)),
        "norm_gain": jnp.clip(1.0 + 0.18 * jax.random.normal(arg_keys[10], (D,), jnp.float32), 0.1, 1.9),
        "up_gate": scatter_about(arg_keys[11], (D, FF), D ** -0.5, 0.125, ((0, 8), (1, 4))),
        "up_value": scatter_about(arg_keys[12], (D, FF), D ** -0.5, 0.125, ((0, 8), (1, 4))),
        "down_weight": scatter_about(arg_keys[13], (D, FF), FF ** -0.5, 0.078125, ((0, 8), (1, 4))),
        "conv_taps": scatter_about(arg_keys[14], (3, 2, FF), 0.6, 3.0, ((2, 4),), jnp.float32),
    }


theta = 10000.0
epsilon = 1e-06

def rotate(values, positions):
    half_dim = values.shape[-1] // 2
    inverse = jnp.power(jnp.float32(theta), -2.0 * jnp.arange(half_dim, dtype=jnp.float32) / values.shape[-1])
    angles = positions[:, None] * inverse[None, :]
    new_shape = (angles.shape[0],) + (1,) * (values.ndim - 2) + (half_dim,)
    cosine = jnp.cos(angles).reshape(new_shape)
    sine_part = jnp.sin(angles).reshape(new_shape)
    floats = values.astype(jnp.float32)
    lower_half = floats[..., :half_dim]
    upper_half = floats[..., half_dim:]
    turned = jnp.concatenate([lower_half * cosine - upper_half * sine_part, lower_half * sine_part + upper_half * cosine], axis=-1)
    return turned.astype(jnp.bfloat16)

def attend(query_turned, key_part, value_part, rope_turned, factor):
    nope_dim = key_part.shape[-1]
    head_count = query_turned.shape[1]
    block_rows = math.gcd(TOKENS, 512)
    grouped = query_turned.reshape(TOKENS // block_rows, block_rows, head_count, query_turned.shape[-1])
    key_float = key_part.astype(jnp.float32)
    rope_float = rope_turned.astype(jnp.float32)
    value_float = value_part.astype(jnp.float32)

    def one_block(query_block):
        query_float = query_block.astype(jnp.float32)
        scores = jnp.einsum('qhd,khd->hqk', query_float[..., :nope_dim], key_float)
        scores = (scores + jnp.einsum('qhd,kd->hqk', query_float[..., nope_dim:], rope_float)) * factor
        row_max = lax.optimization_barrier(jnp.max(scores, axis=-1, keepdims=True))
        weights = jnp.exp(scores - row_max)
        row_total = lax.optimization_barrier(jnp.sum(weights, axis=-1))
        rounded = lax.optimization_barrier(weights.astype(jnp.bfloat16)).astype(jnp.float32)
        weighted = jnp.einsum('hqk,khd->qhd', rounded, value_float)
        return (weighted / jnp.transpose(row_total)[:, :, None]).astype(jnp.bfloat16)
    outputs = lax.map(one_block, grouped)
    return outputs.reshape(TOKENS, head_count * value_part.shape[-1])

def turn_query(queries, head_count, nope_dim, positions):
    shaped = queries.reshape(TOKENS, head_count, nope_dim + ROPE)
    return jnp.concatenate([shaped[..., :nope_dim], rotate(shaped[..., nope_dim:], positions)], axis=-1)

def convolve(values, tap_rows):
    floats = values.astype(jnp.float32)
    zero_row = jnp.zeros((1, floats.shape[1]), jnp.float32)
    before = jnp.concatenate([zero_row, floats[:-1]], axis=0)
    after = jnp.concatenate([floats[1:], zero_row], axis=0)
    return tap_rows[0] * before + tap_rows[1] * floats + tap_rows[2] * after

def reference(residual, query_wide, query_narrow, latent, rope_key, latent_gain, expand_wide, expand_narrow, out_wide, out_narrow, norm_gain, up_gate, up_value, down_weight, conv_taps):
    positions = jnp.arange(TOKENS, dtype=jnp.int32).astype(jnp.float32)
    latent_float = latent.astype(jnp.float32)
    normed_latent = (latent_float * lax.rsqrt(lax.optimization_barrier(jnp.mean(latent_float * latent_float, axis=-1, keepdims=True)) + epsilon) * latent_gain).astype(jnp.bfloat16)
    rope_turned = rotate(rope_key, positions)
    kv_wide = jnp.dot(normed_latent, expand_wide, preferred_element_type=jnp.float32).astype(jnp.bfloat16).reshape(TOKENS, HW, NOPE_W + VAL_W)
    kv_narrow = jnp.dot(normed_latent, expand_narrow, preferred_element_type=jnp.float32).astype(jnp.bfloat16).reshape(TOKENS, HN, NOPE_N + VAL_N)
    query_w = turn_query(query_wide, HW, NOPE_W, positions)
    query_n = turn_query(query_narrow, HN, NOPE_N, positions)
    heads_wide = attend(query_w, kv_wide[..., :NOPE_W], kv_wide[..., NOPE_W:], rope_turned, (NOPE_W + ROPE) ** (-0.5))
    heads_narrow = attend(query_n, kv_narrow[..., :NOPE_N], kv_narrow[..., NOPE_N:], rope_turned, (NOPE_N + ROPE) ** (-0.5))
    wide_cols = HW // N_TP * VAL_W
    narrow_cols = HN // N_TP * VAL_N
    projected = jnp.zeros((TOKENS, D), jnp.float32)
    for group_index in range(N_TP):
        wide_slice = slice(group_index * wide_cols, (group_index + 1) * wide_cols)
        narrow_slice = slice(group_index * narrow_cols, (group_index + 1) * narrow_cols)
        partial_value = jnp.dot(heads_wide[:, wide_slice], out_wide[wide_slice], preferred_element_type=jnp.float32)
        partial_value = partial_value + jnp.dot(heads_narrow[:, narrow_slice], out_narrow[narrow_slice], preferred_element_type=jnp.float32)
        projected = projected + lax.optimization_barrier(partial_value.astype(jnp.bfloat16)).astype(jnp.float32)
    attended = (residual.astype(jnp.float32) + projected).astype(jnp.bfloat16)
    attended_float = attended.astype(jnp.float32)
    factor_rows = lax.rsqrt(lax.optimization_barrier(jnp.mean(attended_float * attended_float, axis=-1, keepdims=True)) + epsilon)
    normed = (attended_float * factor_rows * norm_gain).astype(jnp.bfloat16)
    gate_up = jnp.dot(normed, up_gate, preferred_element_type=jnp.float32).astype(jnp.bfloat16)
    value_up = jnp.dot(normed, up_value, preferred_element_type=jnp.float32).astype(jnp.bfloat16)
    hidden = (jax.nn.silu(convolve(gate_up, conv_taps[:, 0])) * convolve(value_up, conv_taps[:, 1])).astype(jnp.bfloat16)
    unit_cols = FF // N_TP
    channels = jnp.zeros((TOKENS, D), jnp.float32)
    for group_index in range(N_TP):
        unit_slice = slice(group_index * unit_cols, (group_index + 1) * unit_cols)
        partial_value = lax.dot_general(hidden[:, unit_slice], down_weight[:, unit_slice], (((1,), (1,)), ((), ())), preferred_element_type=jnp.float32)
        channels = channels + lax.optimization_barrier(partial_value.astype(jnp.bfloat16)).astype(jnp.float32)
    return (attended_float + channels).astype(jnp.bfloat16)
```

```python
import functools
import math

import jax
import jax.numpy as jnp
import numpy as np
from jax import lax
from jax.experimental import pallas as pl
from jax.experimental.pallas import tpu as pltpu
from jax.sharding import PartitionSpec as P

D = 2048
ROPE = 64
NOPE_W = 128
VAL_W = 128
NOPE_N = 64
VAL_N = 64


theta = 10000.0
epsilon = 1e-06


def padded(block, sides, width):
    for axis, dim in sides:
        count = lax.axis_size(axis)
        forward = [(i, i + 1) for i in range(count - 1)]
        backward = [(target, source) for source, target in forward]
        low = lax.ppermute(
            lax.slice_in_dim(block, block.shape[dim] - width, None, axis=dim), axis, forward
        )
        high = lax.ppermute(lax.slice_in_dim(block, 0, width, axis=dim), axis, backward)
        block = jnp.concatenate([low, block, high], axis=dim)
    return block


def rotate(values, positions):
    half_dim = values.shape[-1] // 2
    inverse = jnp.power(
        jnp.float32(theta), -2.0 * jnp.arange(half_dim, dtype=jnp.float32) / values.shape[-1]
    )
    angles = positions[:, None] * inverse[None, :]
    new_shape = (angles.shape[0],) + (1,) * (values.ndim - 2) + (half_dim,)
    cosine = jnp.cos(angles).reshape(new_shape)
    sine_part = jnp.sin(angles).reshape(new_shape)
    floats = values.astype(jnp.float32)
    lower_half = floats[..., :half_dim]
    upper_half = floats[..., half_dim:]
    turned = jnp.concatenate(
        [
            lower_half * cosine - upper_half * sine_part,
            lower_half * sine_part + upper_half * cosine,
        ],
        axis=-1,
    )
    return turned.astype(jnp.bfloat16)


def turn_query(queries, head_count, nope_dim, positions):
    shaped = queries.reshape(queries.shape[0], head_count, nope_dim + ROPE)
    return jnp.concatenate(
        [shaped[..., :nope_dim], rotate(shaped[..., nope_dim:], positions)], axis=-1
    )


def attend_kernel(scale, chunk, q_ref, k_ref, v_ref, o_ref):
    query = q_ref[0]
    rows = query.shape[0]
    value_dim = v_ref.shape[-1]
    row_max = jnp.full((rows, 1), -1e30, jnp.float32)
    row_total = jnp.zeros((rows, 1), jnp.float32)
    weighted = jnp.zeros((rows, value_dim), jnp.float32)
    for start in range(0, k_ref.shape[1], chunk):
        scores = lax.dot_general(
            query,
            k_ref[0, start : start + chunk, :],
            (((1,), (1,)), ((), ())),
            preferred_element_type=jnp.float32,
        )
        new_max = jnp.maximum(row_max, jnp.max(scores, axis=-1, keepdims=True))
        weights = jnp.exp2((scores - new_max) * scale)
        keep = jnp.exp2((row_max - new_max) * scale)
        row_total = row_total * keep + jnp.sum(weights, axis=-1, keepdims=True)
        weighted = weighted * keep + jnp.dot(
            weights.astype(jnp.bfloat16),
            v_ref[0, start : start + chunk, :],
            preferred_element_type=jnp.float32,
        )
        row_max = new_max
    o_ref[0] = (weighted / row_total).astype(o_ref.dtype)


def attend(query, key, value, factor):
    heads, rows, width = query.shape
    count = key.shape[1]
    value_dim = value.shape[-1]
    block = math.gcd(rows, 320)
    chunk = math.gcd(count, 1024)
    return pl.pallas_call(
        functools.partial(attend_kernel, factor * math.log2(math.e), chunk),
        grid=(heads, rows // block),
        in_specs=[
            pl.BlockSpec((1, block, width), lambda h, i: (h, i, 0)),
            pl.BlockSpec((1, count, width), lambda h, i: (h, 0, 0)),
            pl.BlockSpec((1, count, value_dim), lambda h, i: (h, 0, 0)),
        ],
        out_specs=pl.BlockSpec((1, block, value_dim), lambda h, i: (h, i, 0)),
        out_shape=jax.ShapeDtypeStruct((heads, rows, value_dim), jnp.bfloat16),
        compiler_params=pltpu.CompilerParams(
            dimension_semantics=("arbitrary", "arbitrary"), vmem_limit_bytes=48 << 20
        ),
        cost_estimate=pl.CostEstimate(
            flops=2 * heads * rows * count * 512,
            bytes_accessed=2 * heads * count * (width + value_dim),
            transcendentals=heads * rows * count,
        ),
    )(query, key, value)


def key_value(latent, expand, head_count, key_dim, rope):
    pair = expand.reshape(expand.shape[0], head_count, -1)
    key = jnp.einsum(
        "td,dhn->htn", latent, pair[..., :key_dim], preferred_element_type=jnp.float32
    ).astype(jnp.bfloat16)
    value = jnp.einsum(
        "td,dhn->htn", latent, pair[..., key_dim:], preferred_element_type=jnp.float32
    ).astype(jnp.bfloat16)
    shared = jnp.broadcast_to(rope[None], (head_count,) + rope.shape)
    return jnp.concatenate([key, shared], axis=-1), value


def side_by_side(heads):
    return jnp.transpose(heads, (1, 0, 2)).reshape(heads.shape[1], -1)


def per_device(
    residual,
    query_wide,
    query_narrow,
    latent,
    rope_key,
    latent_gain,
    expand_wide,
    expand_narrow,
    out_wide,
    out_narrow,
    norm_gain,
    up_gate,
    up_value,
    down_weight,
    conv_taps,
):
    tok_rows = residual.shape[0]
    offset = lax.axis_index("sp") * tok_rows
    positions = (offset + lax.iota(jnp.int32, tok_rows)).astype(jnp.float32)
    latent_float = latent.astype(jnp.float32)
    normed_latent = (
        latent_float
        * lax.rsqrt(jnp.mean(latent_float * latent_float, axis=-1, keepdims=True) + epsilon)
        * latent_gain
    ).astype(jnp.bfloat16)
    rope_turned = rotate(rope_key, positions)
    wide_heads = query_wide.shape[1] // (NOPE_W + ROPE)
    narrow_heads = query_narrow.shape[1] // (NOPE_N + ROPE)
    query_w = turn_query(query_wide, wide_heads, NOPE_W, positions)
    query_n = turn_query(query_narrow, narrow_heads, NOPE_N, positions)
    gathered = lax.all_gather(
        jnp.concatenate([normed_latent, rope_turned, jnp.zeros_like(rope_turned)], axis=1),
        "sp",
        axis=0,
        tiled=True,
    )
    full_gain = lax.all_gather(norm_gain, "tp", axis=0, tiled=True)
    gathered, up_gate, up_value, down_weight = lax.optimization_barrier(
        (gathered, up_gate, up_value, down_weight)
    )
    gate_full, value_full, down_full = (
        lax.all_gather(up_gate, "sp", axis=0, tiled=True),
        lax.all_gather(up_value, "sp", axis=0, tiled=True),
        lax.all_gather(down_weight, "sp", axis=0, tiled=True),
    )
    rank = latent.shape[1]
    latent_all, rope_all = gathered[:, :rank], gathered[:, rank : rank + ROPE]
    key_w, value_w = key_value(latent_all, expand_wide, wide_heads, NOPE_W, rope_all)
    key_n, value_n = key_value(latent_all, expand_narrow, narrow_heads, NOPE_N, rope_all)
    heads_wide = side_by_side(
        attend(jnp.transpose(query_w, (1, 0, 2)), key_w, value_w, (NOPE_W + ROPE) ** (-0.5))
    )
    heads_narrow = side_by_side(
        attend(jnp.transpose(query_n, (1, 0, 2)), key_n, value_n, (NOPE_N + ROPE) ** (-0.5))
    )
    head_terms = jnp.dot(heads_wide, out_wide, preferred_element_type=jnp.float32)
    head_terms = head_terms + jnp.dot(heads_narrow, out_narrow, preferred_element_type=jnp.float32)
    head_terms, gate_full, value_full = lax.optimization_barrier(
        (head_terms.astype(jnp.bfloat16), gate_full, value_full)
    )
    head_shares = lax.psum_scatter(
        head_terms, "tp", scatter_dimension=1, tiled=True
    ).astype(jnp.float32)
    attended = (residual.astype(jnp.float32) + head_shares).astype(jnp.bfloat16)
    attended_float = attended.astype(jnp.float32)
    attended_full = lax.all_gather(attended, "tp", axis=1, tiled=True).astype(jnp.float32)
    squares = jnp.mean(attended_full * attended_full, axis=-1, keepdims=True)
    normed_full = (attended_full * lax.rsqrt(squares + epsilon) * full_gain).astype(jnp.bfloat16)
    gate_float = jnp.dot(normed_full, gate_full, preferred_element_type=jnp.float32)
    value_float = jnp.dot(normed_full, value_full, preferred_element_type=jnp.float32)
    gate_width = up_gate.shape[1]
    both_up = jnp.concatenate(
        [gate_float.astype(jnp.bfloat16), value_float.astype(jnp.bfloat16)], axis=1
    )
    extended = padded(both_up, (("sp", 0),), 1).astype(jnp.float32)
    tap_rows = conv_taps.reshape(3, 2 * gate_width)
    smoothed = (
        tap_rows[0] * extended[:-2] + tap_rows[1] * extended[1:-1] + tap_rows[2] * extended[2:]
    )
    hidden = (jax.nn.silu(smoothed[:, :gate_width]) * smoothed[:, gate_width:]).astype(jnp.bfloat16)
    unit_terms = lax.dot_general(
        hidden, down_full, (((1,), (1,)), ((), ())), preferred_element_type=jnp.float32
    )
    unit_shares = lax.psum_scatter(
        unit_terms.astype(jnp.bfloat16), "tp", scatter_dimension=1, tiled=True
    ).astype(jnp.float32)
    return (attended_float + unit_shares).astype(jnp.bfloat16)


MESH = pl.DeviceIdType.MESH
LANES = 128
HALO = 16


def turn_tables(rows, groups):
    half = ROPE // 2
    inverse = np.power(theta, -2.0 * np.arange(half) / ROPE)
    inverse = np.tile(inverse, LANES // half)[None, :]
    local = np.arange(rows)[:, None] * inverse
    start = (np.arange(groups) * rows)[:, None] * inverse
    fine = np.stack([np.cos(local), np.sin(local)]).astype(np.float32)
    coarse = np.stack([np.cos(start), np.sin(start)]).astype(np.float32)
    return fine, coarse


def swap_halves(values, lane):
    half = ROPE // 2
    left = pltpu.roll(values, LANES - half, 1)
    right = pltpu.roll(values, half, 1)
    return jnp.where(lane % ROPE < half, left, right)


def fused_kernel(
    residual,
    query_wide,
    query_narrow,
    latent,
    rope_key,
    latent_gain,
    expand_wide,
    expand_narrow,
    out_wide,
    out_narrow,
    norm_gain,
    up_gate,
    up_value,
    down_weight,
    conv_taps,
    fine_tab,
    coarse_tab,
    output,
    lat_all,
    wts,
    raw_lat,
    raw_rope,
    raw_qw,
    raw_qn,
    qw,
    qn,
    kw,
    vw,
    kn,
    vn,
    accw,
    accn,
    peak,
    expand,
    outcat,
    resid,
    heads,
    part_in,
    xsend,
    xrecv,
    att,
    att_q,
    normed,
    halo,
    gains,
    taps,
    hidden,
    osend,
    orecv,
    result,
    local_sem,
    own_r,
    sib_r,
    x_r,
    xs_r,
    z_s,
    y_s,
    sib_s,
    x_s,
    xs_s,
    wt_r,
    wz_s,
    wy_s,
    ws_s,
    part_r,
    part_s,
    bx_r,
    bx_s,
    swap_r,
    swap_s,
    halo_r,
    halo_s,
    attq_r,
    attq_s,
    gain_r,
    gain_s,
    tap_r,
    tap_s,
    out_r,
    out_s,
):
    sp = lax.axis_index("sp")
    tp = lax.axis_index("tp")
    n_sp = wts.shape[1]
    n_tp = gains.shape[0]
    z, y, x, c = sp // 2, sp % 2, tp // 2, tp % 2
    leader = z % 2
    lead = c == leader
    home = (z // 2 * 2 + c) * 2 + y
    rows, rank = raw_lat.shape
    quarter = rows // n_tp
    weights = (up_gate, up_value, down_weight)
    depth, ff = up_gate.shape
    width = n_sp * depth
    features = resid.shape[1]
    sib = (sp, x * 2 + 1 - c)
    xdev = (sp, (1 - x) * 2 + c)
    ydev = (z * 2 + 1 - y, tp)

    def zflip(a):
        return jnp.where(a == 1, z // 2 * 2 + 1 - z % 2, jnp.where(a == 2, (z + 2) % 4, 3 - z))

    def remote(src, dst, ss, rs, dev):
        return pltpu.make_async_remote_copy(
            src_ref=src, dst_ref=dst, send_sem=ss, recv_sem=rs, device_id=dev, device_id_type=MESH
        )

    barrier = pltpu.get_barrier_semaphore()
    for ds_ in range(n_sp):
        for dt in range(n_tp):
            if ds_ or dt:
                pl.semaphore_signal(
                    barrier,
                    inc=1,
                    device_id=(lax.rem(sp + ds_, n_sp), lax.rem(tp + dt, n_tp)),
                    device_id_type=MESH,
                )

    wide_cols = expand_wide.shape[1]
    loads = [
        (latent, raw_lat),
        (rope_key, raw_rope),
        (query_wide, raw_qw),
        (query_narrow, raw_qn),
        (expand_wide, expand.at[:, pl.ds(0, wide_cols)]),
        (expand_narrow, expand.at[:, pl.ds(wide_cols, expand_narrow.shape[1])]),
        (out_wide, outcat.at[pl.ds(0, out_wide.shape[0])]),
        (out_narrow, outcat.at[pl.ds(out_wide.shape[0], out_narrow.shape[0])]),
        (residual, resid),
    ]
    copies = [
        pltpu.make_async_copy(src, dst, local_sem.at[i]) for i, (src, dst) in enumerate(loads)
    ]
    for copy in copies:
        copy.start()

    lane = lax.broadcasted_iota(jnp.int32, (rows, LANES), 1)
    low = lane < ROPE
    copies[0].wait()
    copies[1].wait()
    base = coarse_tab[:, pl.ds(sp, 1), :]
    cosine = base[0] * fine_tab[0] - base[1] * fine_tab[1]
    sine = base[1] * fine_tab[0] + base[0] * fine_tab[1]
    sine = jnp.where(lane % ROPE < ROPE // 2, -sine, sine)

    def turn(values):
        return values * cosine + swap_halves(values, lane) * sine

    lat_f = raw_lat[...].astype(jnp.float32)
    square = jnp.mean(lat_f * lat_f, axis=-1, keepdims=True)
    lat_all[sp, :, 0:rank] = (lat_f * lax.rsqrt(square + epsilon) * latent_gain[...]).astype(
        jnp.bfloat16
    )
    rope_f = raw_rope[...].astype(jnp.float32)
    rope_f = jnp.concatenate([rope_f, rope_f], axis=1)
    lat_all[sp, :, rank:] = turn(rope_f).astype(jnp.bfloat16)

    pl.semaphore_wait(barrier, n_sp * n_tp - 1)

    def piece(owner, who):
        return lat_all.at[owner, pl.ds(pl.multiple_of(who * quarter, quarter), quarter)]

    def z_copy(a):
        return remote(
            piece(sp, tp), piece(sp, tp), z_s.at[a - 1], own_r.at[a + 1], (zflip(a) * 2 + y, tp)
        )

    def owner_of(i):
        b = jnp.where((i == 1) | (i >= 5), 1, 0)
        a = jnp.where(i <= 1, 0, jnp.where(i <= 4, i - 1, i - 4))
        oz = jnp.where(a == 0, z, zflip(a))
        return oz * 2 + jnp.where(b == 1, 1 - y, y)

    def y_copy(i):
        own = piece(owner_of(i), tp)
        return remote(own, own, y_s.at[i], own_r.at[jnp.where(i == 0, 1, i + 3)], ydev)

    def sib_copy(i):
        own = piece(owner_of(i), tp)
        return remote(own, own, sib_s.at[i], sib_r.at[i], sib)

    def x_copy(i):
        own = piece(owner_of(i), tp)
        return remote(own, own, x_s.at[i], x_r.at[i], xdev)

    def xs_copy(i):
        other = piece(owner_of(i), (1 - x) * 2 + c)
        return remote(other, other, xs_s.at[i], xs_r.at[i], sib)

    def stage_one(i):
        y_arrival = piece(owner_of(i), tp)
        remote(y_arrival, y_arrival, y_s.at[0], own_r.at[i], sib).wait_recv()
        x_copy(i).start()
        sib_copy(i).start()

    def stage_two(i):
        x_copy(i).wait_recv()
        xs_copy(i).start()

    y_copy(0).start()
    for a in (1, 2, 3):
        z_copy(a).start()

    def z_weight(m, slot, a):
        return remote(
            weights[m],
            wts.at[m, sp],
            wz_s.at[m, slot],
            wt_r.at[m, a + 1],
            (zflip(a) * 2 + y, tp),
        )

    def y_weight(m, k):
        spk = owner_of(k)
        src = weights[m] if isinstance(k, int) and k == 0 else wts.at[m, spk]
        there = 1 if isinstance(k, int) and k == 0 else k + 3
        return remote(src, wts.at[m, spk], wy_s.at[m, k], wt_r.at[m, there], ydev)

    def sib_weight(m, k):
        spk = owner_of(k)
        src = weights[m] if isinstance(k, int) and k == 0 else wts.at[m, spk]
        return remote(src, wts.at[m, spk], ws_s.at[m, k], wt_r.at[m, k], sib)

    def own_weight(m):
        return pltpu.make_async_copy(weights[m], wts.at[m, sp], wt_r.at[m, 0])

    def wait_weight(m, k):
        ref = wts.at[m, owner_of(k)]
        remote(ref, ref, wy_s.at[m, 0], wt_r.at[m, k], sib).wait_recv()

    for m in range(3):

        @pl.when(lead)
        def _():
            z_weight(m, 0, 2).start()

        @pl.when(jnp.logical_not(lead))
        def _():
            z_weight(m, 0, 1).start()
            z_weight(m, 1, 3).start()

    gains[tp] = norm_gain[...]
    gain_peers = [(sp, lax.rem(tp + d, n_tp)) for d in range(1, n_tp)]

    def gain_copy(d):
        return remote(
            norm_gain, gains.at[tp], gain_s.at[d], gain_r.at[d], (sp, lax.rem(tp + d + 1, n_tp))
        )

    for d in range(n_tp - 1):
        gain_copy(d).start()

    def tap_copy():
        return remote(conv_taps, taps, tap_s.at[0], tap_r.at[0], sib)

    @pl.when(lead)
    def _():
        tap_copy().start()
        taps[...] = conv_taps[...]

    copies[2].wait()
    copies[3].wait()
    one = raw_qw[:, LANES : 2 * LANES].astype(jnp.float32)
    two = raw_qw[:, 2 * LANES :].astype(jnp.float32)
    turned_two = turn(two)
    qw[0, :, 0:LANES] = raw_qw[:, 0:LANES]
    qw[0, :, LANES:] = jnp.where(low, turn(one), 0.0).astype(jnp.bfloat16)
    qw[1, :, 0:LANES] = jnp.where(
        low, pltpu.roll(one, ROPE, 1), pltpu.roll(two, ROPE, 1)
    ).astype(jnp.bfloat16)
    qw[1, :, LANES:] = jnp.where(low, pltpu.roll(turned_two, ROPE, 1), 0.0).astype(jnp.bfloat16)
    for h in range(2):
        tile = raw_qn[:, h * LANES : (h + 1) * LANES].astype(jnp.float32)
        qn[h] = jnp.where(low, tile, turn(tile)).astype(jnp.bfloat16)
        vw[h, :, LANES:] = jnp.ones((rows, LANES), jnp.bfloat16)
    peak[...] = jnp.full(peak.shape, -1e30, jnp.float32)
    accw[...] = jnp.zeros(accw.shape, jnp.float32)
    accn[...] = jnp.zeros(accn.shape, jnp.float32)
    for i in (4, 5, 6, 7, 8):
        copies[i].wait()

    tile_rows = rows // 2

    def attend_tile(slot, query, key, value, acc, at, scale):
        scores = lax.dot_general(
            query, key, (((1,), (1,)), ((), ())), preferred_element_type=jnp.float32
        )
        before = peak[slot, at, :]
        after = jnp.maximum(before, jnp.max(scores, axis=-1, keepdims=True))
        pieces = [
            jnp.exp2((scores[:, j : j + LANES] - after) * scale)
            for j in range(0, scores.shape[1], LANES)
        ]
        spread = jnp.concatenate(pieces, axis=1).astype(jnp.bfloat16)
        keep = jnp.exp2((before - after) * scale)
        new = jnp.dot(spread, value, preferred_element_type=jnp.float32)
        for j in range(0, new.shape[1], LANES):
            acc[at, j : j + LANES] = acc[at, j : j + LANES] * keep + new[:, j : j + LANES]
        peak[slot, at, :] = after

    scale_w = (NOPE_W + ROPE) ** (-0.5) * math.log2(math.e)
    scale_n = (NOPE_N + ROPE) ** (-0.5) * math.log2(math.e)

    def block_step(i, carry):
        @pl.when(i == 1)
        def _():
            stage_one(i)
            stage_one(i + 1)
            stage_two(i)
            y_copy(i + 1).start()

        @pl.when((i >= 1) & (i <= 5))
        def _():
            stage_one(i + 2)

        @pl.when((i >= 1) & (i <= 2))
        def _():
            y_copy(i + 2).start()

        @pl.when((i >= 1) & (i <= 6))
        def _():
            stage_two(i + 1)

        @pl.when((i == 3) & lead)
        def _():
            for m in range(3):
                y_weight(m, 0).start()
                sib_weight(m, 0).start()
                own_weight(m).start()

        @pl.when(i >= 1)
        def _():
            sib_copy(i).wait_recv()
            xs_copy(i).wait_recv()

        owner = owner_of(i)
        shared = lat_all[owner, :, 0:rank]
        rope = lat_all[owner, :, rank:].astype(jnp.float32)
        for h in range(2):
            pair = jnp.dot(
                shared,
                expand[:, h * 2 * LANES : (h + 1) * 2 * LANES],
                preferred_element_type=jnp.float32,
            )
            kw[h, :, 0:LANES] = pair[:, 0:LANES].astype(jnp.bfloat16)
            kw[h, :, LANES:] = lat_all[owner, :, rank:]
            vw[h, :, 0:LANES] = pair[:, LANES:].astype(jnp.bfloat16)
        pair = jnp.dot(shared, expand[:, wide_cols:], preferred_element_type=jnp.float32)
        for h in range(2):
            mine = pair[:, h * LANES : (h + 1) * LANES]
            kn[h] = jnp.where(low, mine, rope).astype(jnp.bfloat16)
            vn[h] = jnp.where(low, 1.0, mine).astype(jnp.bfloat16)
        for t in range(rows // tile_rows):
            at = pl.ds(t * tile_rows, tile_rows)
            for h in range(2):
                attend_tile(h, qw[h, at, :], kw[h], vw[h], accw.at[h], at, scale_w)
                attend_tile(2 + h, qn[h, at, :], kn[h], vn[h], accn.at[h], at, scale_n)
        return carry

    lax.fori_loop(0, n_sp, block_step, 0)

    for h in range(2):
        heads[:, h * LANES : (h + 1) * LANES] = (
            accw[h, :, 0:LANES] / accw[h, :, LANES:]
        ).astype(jnp.bfloat16)
    first, second = accn[0], accn[1]
    first_r, second_r = pltpu.roll(first, ROPE, 1), pltpu.roll(second, ROPE, 1)
    heads[:, 2 * LANES :] = (
        jnp.where(low, first_r, second) / jnp.where(low, first, second_r)
    ).astype(jnp.bfloat16)

    step_rows = LANES
    n_steps = rows // step_rows

    def tile_at(t):
        return pl.ds(pl.multiple_of(t * step_rows, step_rows), step_rows)

    def part_copy(t):
        return remote(
            xsend.at[tile_at(t)], part_in.at[tile_at(t)], part_s.at[t], part_r.at[t], sib
        )

    def bx_copy(t):
        return remote(xsend.at[tile_at(t)], xrecv.at[tile_at(t)], bx_s.at[t], bx_r.at[t], xdev)

    pair_dev = (zflip(1) * 2 + y, tp)

    def swap_copy(t):
        return remote(att.at[tile_at(t)], att.at[tile_at(t)], swap_s.at[t], swap_r.at[t], pair_dev)

    def project(t, carry):
        at = tile_at(t)
        pieces = []
        for j in range(n_tp):
            cols = slice(j * features, (j + 1) * features)
            term = jnp.dot(heads[at, :], outcat[:, cols], preferred_element_type=jnp.float32)
            mine = jnp.where(tp == j, 1.0, 0.0)
            pieces.append(term + resid[at, :].astype(jnp.float32) * mine)

        @pl.when(jnp.logical_not(lead))
        def _():
            for j in range(n_tp):
                cols = slice(j * features, (j + 1) * features)
                xsend[at, cols] = pieces[j].astype(jnp.bfloat16)
            part_copy(t).start()

        @pl.when(lead)
        def _():
            part_copy(t).wait_recv()
            for j in range(n_tp):
                cols = slice(j * features, (j + 1) * features)
                xsend[at, cols] = (
                    pieces[j] + part_in[at, cols].astype(jnp.float32)
                ).astype(jnp.bfloat16)
            bx_copy(t).start()

        return carry

    lax.fori_loop(0, n_steps, project, 0)

    def forward_z(m):
        for k in (2, 3, 4):
            wait_weight(m, k)
            y_weight(m, k).start()
            sib_weight(m, k).start()

    def forward_y(m):
        for k in (1, 5, 6, 7):
            wait_weight(m, k)
            sib_weight(m, k).start()

    def halo_copy(side, plane):
        there = sp - 1 if side == 1 else sp + 1
        tz, ty = there // 2, there % 2
        src = att.at[pl.ds(0, HALO)] if side == 1 else att.at[pl.ds(rows - HALO, HALO)]
        dev = ((tz // 2 * 2 + plane) * 2 + ty, x * 2 + tz % 2)
        return remote(src, halo.at[side], halo_s.at[side, plane], halo_r.at[side], dev)

    def attq_copy(col):
        return remote(
            att.at[:, pl.ds(pl.multiple_of(col * features, features), features)],
            att_q,
            attq_s.at[0],
            attq_r.at[0],
            sib,
        )

    @pl.when(lead)
    def _():
        forward_z(0)

        def exchange(t, carry):
            at = tile_at(t)
            bx_copy(t).wait_recv()
            att[at, :] = (
                xsend[at, :].astype(jnp.float32) + xrecv[at, :].astype(jnp.float32)
            ).astype(jnp.bfloat16)
            swap_copy(t).start()
            return carry

        lax.fori_loop(0, n_steps, exchange, 0)

        @pl.when(sp > 0)
        def _():
            for plane in range(2):
                halo_copy(1, plane).start()

        @pl.when(sp < n_sp - 1)
        def _():
            for plane in range(2):
                halo_copy(0, plane).start()

        attq_copy(x * 2 + 1 - c).start()
        att_q[...] = att[:, pl.ds(pl.multiple_of(tp * features, features), features)]
        forward_z(1)
        forward_y(0)

    @pl.when(jnp.logical_not(lead))
    def _():
        for t in range(n_steps):
            swap_copy(t).wait_recv()

    for d in range(n_tp - 1):
        gain_copy(d).wait_recv()

    def normalize(values):
        values = values.astype(jnp.float32)
        factor = lax.rsqrt(jnp.mean(values * values, axis=-1, keepdims=True) + epsilon)
        return jnp.concatenate(
            [
                values[:, j * features : (j + 1) * features] * factor * gains[j]
                for j in range(n_tp)
            ],
            axis=1,
        )

    def norm_step(t, carry):
        normed[tile_at(t), :] = normalize(att[tile_at(t), :]).astype(jnp.bfloat16)
        return carry

    lax.fori_loop(0, n_steps, norm_step, 0)

    def halo_wait(side):
        remote(
            halo.at[side], halo.at[side], halo_s.at[side, 0], halo_r.at[side], sib
        ).wait_recv()

    @pl.when(home > 0)
    def _():
        halo_wait(0)

    @pl.when(home < n_sp - 1)
    def _():
        halo_wait(1)

    previous = jnp.where(home > 0, normalize(halo[0])[HALO - 1 :, :], 0.0)
    following = jnp.where(home < n_sp - 1, normalize(halo[1])[0:1, :], 0.0)
    edge = lax.broadcasted_iota(jnp.int32, (HALO, width), 0)
    normed[rows:, :] = jnp.where(
        edge == 0, previous, jnp.where(edge == 1, following, 0.0)
    ).astype(jnp.bfloat16)

    @pl.when(lead)
    def _():
        forward_y(1)
        wait_weight(0, 0)
        wait_weight(1, 0)

    @pl.when(jnp.logical_not(lead))
    def _():
        tap_copy().wait_recv()
        for m in range(2):
            for k in range(n_sp):
                wait_weight(m, k)

    def smooth(values, cols, which):
        size = values.shape[1]
        row = lax.broadcasted_iota(jnp.int32, (rows, size), 0)
        values = values.astype(jnp.bfloat16).astype(jnp.float32)
        main = values[0:rows]
        before = jnp.where(row == 0, values[rows : rows + 1], pltpu.roll(main, 1, 0))
        after = jnp.where(
            row == rows - 1, values[rows + 1 : rows + 2], pltpu.roll(main, rows - 1, 0)
        )
        return (
            taps[0, which : which + 1, cols] * before
            + taps[1, which : which + 1, cols] * main
            + taps[2, which : which + 1, cols] * after
        )

    def mix(start, size):
        cols = pl.ds(start, size)
        both = []
        for m in range(2):
            rhs = wts[m, :, :, cols].reshape(width, size)
            both.append(
                smooth(jnp.dot(normed[...], rhs, preferred_element_type=jnp.float32), cols, m)
            )
        gate = both[0]
        hidden[:, cols] = (gate / (1.0 + jnp.exp(-gate)) * both[1]).astype(jnp.bfloat16)

    block = 2 * LANES

    def mix_step(j, carry):
        mix(pl.multiple_of(j * block, block), block)
        return carry

    lax.fori_loop(0, ff // block, mix_step, 0)
    if ff % block:
        mix(ff // block * block, ff % block)

    @pl.when(lead)
    def _():
        forward_z(2)

    parts = features // depth
    source = leader * 2 + x

    def out_copy(i, owner):
        dev_tp = owner // parts
        half = owner % parts
        return remote(
            osend.at[i],
            orecv.at[source, :, pl.ds(pl.multiple_of(half * depth, depth), depth)],
            out_s.at[i],
            out_r.at[source, half],
            (home, dev_tp),
        )

    def mine(owner):
        return (home == sp) & (owner // parts == tp)

    def down_step(i, carry):
        @pl.when(lead & ((i == 1) | (i >= 5)))
        def _():
            wait_weight(2, i)
            sib_weight_any(2, i).start()

        @pl.when(jnp.logical_not(lead) | (i == 0))
        def _():
            wait_weight(2, i)

        owner = owner_of(i)
        term = lax.dot_general(
            hidden[...],
            wts[2, owner],
            (((1,), (1,)), ((), ())),
            preferred_element_type=jnp.float32,
        ).astype(jnp.bfloat16)

        @pl.when(mine(owner))
        def _():
            half = owner % parts
            orecv[source, :, pl.ds(pl.multiple_of(half * depth, depth), depth)] = term

        @pl.when(jnp.logical_not(mine(owner)))
        def _():
            osend[i] = term
            out_copy(i, owner).start()

        return carry

    def sib_weight_any(m, k):
        spk = owner_of(k)
        return remote(wts.at[m, spk], wts.at[m, spk], ws_s.at[m, k], wt_r.at[m, k], sib)

    lax.fori_loop(0, n_sp, down_step, 0)

    @pl.when(jnp.logical_not(lead))
    def _():
        attq_copy(0).wait_recv()

    for s in range(orecv.shape[0]):

        @pl.when(jnp.logical_not(lead & (s == source)))
        def _():
            for half in range(parts):
                ref = orecv.at[s, :, pl.ds(half * depth, depth)]
                remote(ref, ref, out_s.at[0], out_r.at[s, half], sib).wait_recv()

    total = att_q[...].astype(jnp.float32)
    for s in range(orecv.shape[0]):
        total = total + orecv[s].astype(jnp.float32)
    result[...] = total.astype(jnp.bfloat16)
    store = pltpu.make_async_copy(result, output, local_sem.at[0])
    store.start()

    y_copy(0).wait_send()
    for i in (2, 3, 4):
        y_copy(i).wait_send()
    for a in (1, 2, 3):
        z_copy(a).wait_send()
    for i in range(1, n_sp):
        x_copy(i).wait_send()
        sib_copy(i).wait_send()
        xs_copy(i).wait_send()
    for d in range(n_tp - 1):
        gain_copy(d).wait_send()

    @pl.when(lead)
    def _():
        tap_copy().wait_send()
        attq_copy(0).wait_send()
        for m in range(3):
            z_weight(m, 0, 2).wait_send()
            for k in (0, 2, 3, 4):
                y_weight(m, k).wait_send()
            for k in range(n_sp):
                sib_weight(m, k).wait_send()
        for t in range(n_steps):
            bx_copy(t).wait_send()
            swap_copy(t).wait_send()

        @pl.when(sp > 0)
        def _():
            for plane in range(2):
                halo_copy(1, plane).wait_send()

        @pl.when(sp < n_sp - 1)
        def _():
            for plane in range(2):
                halo_copy(0, plane).wait_send()

    @pl.when(jnp.logical_not(lead))
    def _():
        for m in range(3):
            z_weight(m, 0, 1).wait_send()
            z_weight(m, 1, 3).wait_send()
        for t in range(n_steps):
            part_copy(t).wait_send()

    def out_wait(i, carry):
        owner = owner_of(i)

        @pl.when(jnp.logical_not(mine(owner)))
        def _():
            out_copy(i, owner).wait_send()

        return carry

    lax.fori_loop(0, n_sp, out_wait, 0)
    store.wait()


def fused_device(n_sp, n_tp, *arrays):
    (
        residual,
        query_wide,
        query_narrow,
        latent,
        rope_key,
        latent_gain,
        expand_wide,
        expand_narrow,
        out_wide,
        out_narrow,
        norm_gain,
        up_gate,
        up_value,
        down_weight,
        conv_taps,
    ) = arrays
    rows, features = residual.shape
    rank = latent.shape[1]
    depth, ff = up_gate.shape
    width = n_sp * depth
    fine, coarse = turn_tables(rows, n_sp)
    operands = (
        residual,
        query_wide,
        query_narrow,
        latent,
        rope_key,
        latent_gain[None],
        expand_wide,
        expand_narrow,
        out_wide,
        out_narrow,
        norm_gain[None],
        up_gate,
        up_value,
        down_weight,
        conv_taps,
        jnp.asarray(fine),
        jnp.asarray(coarse),
    )
    small = (5, 10, 14, 15, 16)
    anywhere = pl.BlockSpec(memory_space=pl.ANY)
    inside = pl.BlockSpec(memory_space=pltpu.VMEM)
    low, full = jnp.bfloat16, jnp.float32
    buffers = [
        ((n_sp, rows, rank + LANES), low),
        ((3, n_sp, depth, ff), low),
        ((rows, rank), low),
        ((rows, ROPE), low),
        (query_wide.shape, low),
        (query_narrow.shape, low),
        ((2, rows, 2 * LANES), low),
        ((2, rows, LANES), low),
        ((2, rows, 2 * LANES), low),
        ((2, rows, 2 * LANES), low),
        ((2, rows, LANES), low),
        ((2, rows, LANES), low),
        ((2, rows, 2 * LANES), full),
        ((2, rows, LANES), full),
        ((4, rows, LANES), full),
        ((rank, expand_wide.shape[1] + expand_narrow.shape[1]), low),
        ((out_wide.shape[0] + out_narrow.shape[0], width), low),
        ((rows, features), low),
        ((rows, out_wide.shape[0] + out_narrow.shape[0]), low),
        ((rows, width), low),
        ((rows, width), low),
        ((rows, width), low),
        ((rows, width), low),
        ((rows, features), low),
        ((rows + HALO, width), low),
        ((2, HALO, width), low),
        ((n_tp, 1, features), full),
        (conv_taps.shape, full),
        ((rows, ff), low),
        ((n_sp, rows, depth), low),
        ((4, rows, features), low),
        ((rows, features), low),
    ]
    steps = rows // LANES
    semaphores = [
        (9,),
        (8,),
        (8,),
        (8,),
        (8,),
        (3,),
        (5,),
        (8,),
        (8,),
        (8,),
        (3, 8),
        (3, 2),
        (3, 5),
        (3, 8),
        (steps,),
        (steps,),
        (steps,),
        (steps,),
        (steps,),
        (steps,),
        (2,),
        (2, 2),
        (1,),
        (1,),
        (3,),
        (3,),
        (1,),
        (1,),
        (4, features // depth),
        (8,),
    ]
    return pl.pallas_call(
        fused_kernel,
        out_shape=jax.ShapeDtypeStruct((rows, features), jnp.bfloat16),
        in_specs=[inside if i in small else anywhere for i in range(len(operands))],
        out_specs=anywhere,
        scratch_shapes=[pltpu.VMEM(shape, dtype) for shape, dtype in buffers]
        + [pltpu.SemaphoreType.DMA(shape) for shape in semaphores],
        compiler_params=pltpu.CompilerParams(
            collective_id=0, has_side_effects=True, vmem_limit_bytes=67043328
        ),
    )(*operands)


def solution(mesh):
    in_specs = (
        P("sp", "tp"),
        P("sp", "tp"),
        P("sp", "tp"),
        P("sp", None),
        P("sp", None),
        P(),
        P(None, "tp"),
        P(None, "tp"),
        P("tp", None),
        P("tp", None),
        P("tp"),
        P("sp", "tp"),
        P("sp", "tp"),
        P("sp", "tp"),
        P(None, None, "tp"),
    )
    out_specs = P("sp", "tp")
    n_sp, n_tp = mesh.shape["sp"], mesh.shape["tp"]
    body = per_device
    if (n_sp, n_tp) == (8, 4):
        body = functools.partial(fused_device, n_sp, n_tp)
    return jax.shard_map(
        body, mesh=mesh, in_specs=in_specs, out_specs=out_specs, check_vma=False
    )
```

```python
import functools
import math

import jax
import jax.numpy as jnp
import numpy as np
from jax import lax
from jax.experimental import pallas as pl
from jax.experimental.pallas import tpu as pltpu
from jax.sharding import PartitionSpec as P

D = 2048
ROPE = 64
NOPE_W = 128
VAL_W = 128
NOPE_N = 64
VAL_N = 64


theta = 10000.0
epsilon = 1e-06


def padded(block, sides, width):
    for axis, dim in sides:
        count = lax.axis_size(axis)
        forward = [(i, i + 1) for i in range(count - 1)]
        backward = [(target, source) for source, target in forward]
        low = lax.ppermute(
            lax.slice_in_dim(block, block.shape[dim] - width, None, axis=dim), axis, forward
        )
        high = lax.ppermute(lax.slice_in_dim(block, 0, width, axis=dim), axis, backward)
        block = jnp.concatenate([low, block, high], axis=dim)
    return block


def rotate(values, positions):
    half_dim = values.shape[-1] // 2
    inverse = jnp.power(
        jnp.float32(theta), -2.0 * jnp.arange(half_dim, dtype=jnp.float32) / values.shape[-1]
    )
    angles = positions[:, None] * inverse[None, :]
    new_shape = (angles.shape[0],) + (1,) * (values.ndim - 2) + (half_dim,)
    cosine = jnp.cos(angles).reshape(new_shape)
    sine_part = jnp.sin(angles).reshape(new_shape)
    floats = values.astype(jnp.float32)
    lower_half = floats[..., :half_dim]
    upper_half = floats[..., half_dim:]
    turned = jnp.concatenate(
        [
            lower_half * cosine - upper_half * sine_part,
            lower_half * sine_part + upper_half * cosine,
        ],
        axis=-1,
    )
    return turned.astype(jnp.bfloat16)


def turn_query(queries, head_count, nope_dim, positions):
    shaped = queries.reshape(queries.shape[0], head_count, nope_dim + ROPE)
    return jnp.concatenate(
        [shaped[..., :nope_dim], rotate(shaped[..., nope_dim:], positions)], axis=-1
    )


def attend_kernel(scale, chunk, q_ref, k_ref, v_ref, o_ref):
    query = q_ref[0]
    rows = query.shape[0]
    value_dim = v_ref.shape[-1]
    row_max = jnp.full((rows, 1), -1e30, jnp.float32)
    row_total = jnp.zeros((rows, 1), jnp.float32)
    weighted = jnp.zeros((rows, value_dim), jnp.float32)
    for start in range(0, k_ref.shape[1], chunk):
        scores = lax.dot_general(
            query,
            k_ref[0, start : start + chunk, :],
            (((1,), (1,)), ((), ())),
            preferred_element_type=jnp.float32,
        )
        new_max = jnp.maximum(row_max, jnp.max(scores, axis=-1, keepdims=True))
        weights = jnp.exp2((scores - new_max) * scale)
        keep = jnp.exp2((row_max - new_max) * scale)
        row_total = row_total * keep + jnp.sum(weights, axis=-1, keepdims=True)
        weighted = weighted * keep + jnp.dot(
            weights.astype(jnp.bfloat16),
            v_ref[0, start : start + chunk, :],
            preferred_element_type=jnp.float32,
        )
        row_max = new_max
    o_ref[0] = (weighted / row_total).astype(o_ref.dtype)


def attend(query, key, value, factor):
    heads, rows, width = query.shape
    count = key.shape[1]
    value_dim = value.shape[-1]
    block = math.gcd(rows, 320)
    chunk = math.gcd(count, 1024)
    return pl.pallas_call(
        functools.partial(attend_kernel, factor * math.log2(math.e), chunk),
        grid=(heads, rows // block),
        in_specs=[
            pl.BlockSpec((1, block, width), lambda h, i: (h, i, 0)),
            pl.BlockSpec((1, count, width), lambda h, i: (h, 0, 0)),
            pl.BlockSpec((1, count, value_dim), lambda h, i: (h, 0, 0)),
        ],
        out_specs=pl.BlockSpec((1, block, value_dim), lambda h, i: (h, i, 0)),
        out_shape=jax.ShapeDtypeStruct((heads, rows, value_dim), jnp.bfloat16),
        compiler_params=pltpu.CompilerParams(
            dimension_semantics=("arbitrary", "arbitrary"), vmem_limit_bytes=48 << 20
        ),
        cost_estimate=pl.CostEstimate(
            flops=2 * heads * rows * count * 512,
            bytes_accessed=2 * heads * count * (width + value_dim),
            transcendentals=heads * rows * count,
        ),
    )(query, key, value)


def key_value(latent, expand, head_count, key_dim, rope):
    pair = expand.reshape(expand.shape[0], head_count, -1)
    key = jnp.einsum(
        "td,dhn->htn", latent, pair[..., :key_dim], preferred_element_type=jnp.float32
    ).astype(jnp.bfloat16)
    value = jnp.einsum(
        "td,dhn->htn", latent, pair[..., key_dim:], preferred_element_type=jnp.float32
    ).astype(jnp.bfloat16)
    shared = jnp.broadcast_to(rope[None], (head_count,) + rope.shape)
    return jnp.concatenate([key, shared], axis=-1), value


def side_by_side(heads):
    return jnp.transpose(heads, (1, 0, 2)).reshape(heads.shape[1], -1)


def per_device(
    residual,
    query_wide,
    query_narrow,
    latent,
    rope_key,
    latent_gain,
    expand_wide,
    expand_narrow,
    out_wide,
    out_narrow,
    norm_gain,
    up_gate,
    up_value,
    down_weight,
    conv_taps,
):
    tok_rows = residual.shape[0]
    offset = lax.axis_index("sp") * tok_rows
    positions = (offset + lax.iota(jnp.int32, tok_rows)).astype(jnp.float32)
    latent_float = latent.astype(jnp.float32)
    normed_latent = (
        latent_float
        * lax.rsqrt(jnp.mean(latent_float * latent_float, axis=-1, keepdims=True) + epsilon)
        * latent_gain
    ).astype(jnp.bfloat16)
    rope_turned = rotate(rope_key, positions)
    wide_heads = query_wide.shape[1] // (NOPE_W + ROPE)
    narrow_heads = query_narrow.shape[1] // (NOPE_N + ROPE)
    query_w = turn_query(query_wide, wide_heads, NOPE_W, positions)
    query_n = turn_query(query_narrow, narrow_heads, NOPE_N, positions)
    gathered = lax.all_gather(
        jnp.concatenate([normed_latent, rope_turned, jnp.zeros_like(rope_turned)], axis=1),
        "sp",
        axis=0,
        tiled=True,
    )
    full_gain = lax.all_gather(norm_gain, "tp", axis=0, tiled=True)
    gathered, up_gate, up_value, down_weight = lax.optimization_barrier(
        (gathered, up_gate, up_value, down_weight)
    )
    gate_full, value_full, down_full = (
        lax.all_gather(up_gate, "sp", axis=0, tiled=True),
        lax.all_gather(up_value, "sp", axis=0, tiled=True),
        lax.all_gather(down_weight, "sp", axis=0, tiled=True),
    )
    rank = latent.shape[1]
    latent_all, rope_all = gathered[:, :rank], gathered[:, rank : rank + ROPE]
    key_w, value_w = key_value(latent_all, expand_wide, wide_heads, NOPE_W, rope_all)
    key_n, value_n = key_value(latent_all, expand_narrow, narrow_heads, NOPE_N, rope_all)
    heads_wide = side_by_side(
        attend(jnp.transpose(query_w, (1, 0, 2)), key_w, value_w, (NOPE_W + ROPE) ** (-0.5))
    )
    heads_narrow = side_by_side(
        attend(jnp.transpose(query_n, (1, 0, 2)), key_n, value_n, (NOPE_N + ROPE) ** (-0.5))
    )
    head_terms = jnp.dot(heads_wide, out_wide, preferred_element_type=jnp.float32)
    head_terms = head_terms + jnp.dot(heads_narrow, out_narrow, preferred_element_type=jnp.float32)
    head_terms, gate_full, value_full = lax.optimization_barrier(
        (head_terms.astype(jnp.bfloat16), gate_full, value_full)
    )
    head_shares = lax.psum_scatter(
        head_terms, "tp", scatter_dimension=1, tiled=True
    ).astype(jnp.float32)
    attended = (residual.astype(jnp.float32) + head_shares).astype(jnp.bfloat16)
    attended_float = attended.astype(jnp.float32)
    attended_full = lax.all_gather(attended, "tp", axis=1, tiled=True).astype(jnp.float32)
    squares = jnp.mean(attended_full * attended_full, axis=-1, keepdims=True)
    normed_full = (attended_full * lax.rsqrt(squares + epsilon) * full_gain).astype(jnp.bfloat16)
    gate_float = jnp.dot(normed_full, gate_full, preferred_element_type=jnp.float32)
    value_float = jnp.dot(normed_full, value_full, preferred_element_type=jnp.float32)
    gate_width = up_gate.shape[1]
    both_up = jnp.concatenate(
        [gate_float.astype(jnp.bfloat16), value_float.astype(jnp.bfloat16)], axis=1
    )
    extended = padded(both_up, (("sp", 0),), 1).astype(jnp.float32)
    tap_rows = conv_taps.reshape(3, 2 * gate_width)
    smoothed = (
        tap_rows[0] * extended[:-2] + tap_rows[1] * extended[1:-1] + tap_rows[2] * extended[2:]
    )
    hidden = (jax.nn.silu(smoothed[:, :gate_width]) * smoothed[:, gate_width:]).astype(jnp.bfloat16)
    unit_terms = lax.dot_general(
        hidden, down_full, (((1,), (1,)), ((), ())), preferred_element_type=jnp.float32
    )
    unit_shares = lax.psum_scatter(
        unit_terms.astype(jnp.bfloat16), "tp", scatter_dimension=1, tiled=True
    ).astype(jnp.float32)
    return (attended_float + unit_shares).astype(jnp.bfloat16)


MESH = pl.DeviceIdType.MESH
LANES = 128
HALO = 16


def turn_tables(rows, groups):
    half = ROPE // 2
    inverse = np.power(theta, -2.0 * np.arange(half) / ROPE)
    inverse = np.tile(inverse, LANES // half)[None, :]
    local = np.arange(rows)[:, None] * inverse
    start = (np.arange(groups) * rows)[:, None] * inverse
    fine = np.stack([np.cos(local), np.sin(local)]).astype(np.float32)
    coarse = np.stack([np.cos(start), np.sin(start)]).astype(np.float32)
    return fine, coarse


def swap_halves(values, lane):
    half = ROPE // 2
    left = pltpu.roll(values, LANES - half, 1)
    right = pltpu.roll(values, half, 1)
    return jnp.where(lane % ROPE < half, left, right)


def fused_kernel(
    residual,
    query_wide,
    query_narrow,
    latent,
    rope_key,
    latent_gain,
    expand_wide,
    expand_narrow,
    out_wide,
    out_narrow,
    norm_gain,
    up_gate,
    up_value,
    down_weight,
    conv_taps,
    fine_tab,
    coarse_tab,
    output,
    lat_all,
    wts,
    raw_lat,
    raw_rope,
    raw_qw,
    raw_qn,
    qw,
    qn,
    kw,
    vw,
    kn,
    vn,
    accw,
    accn,
    peak,
    expand,
    outcat,
    resid,
    heads,
    part_in,
    xsend,
    xrecv,
    att,
    att_q,
    normed,
    halo,
    gains,
    taps,
    hidden,
    osend,
    orx,
    orecv,
    result,
    local_sem,
    own_r,
    sib_r,
    x_r,
    xs_r,
    z_s,
    y_s,
    sib_s,
    x_s,
    xs_s,
    wt_r,
    wz_s,
    wy_s,
    ws_s,
    part_r,
    part_s,
    bx_r,
    bx_s,
    swap_r,
    swap_s,
    cross_r,
    cross_s,
    halo_r,
    halo_s,
    attq_r,
    attq_s,
    gain_r,
    gain_s,
    tap_r,
    tap_s,
    ox_r,
    ox_s,
    out_r,
    out_s,
):
    sp = lax.axis_index("sp")
    tp = lax.axis_index("tp")
    n_sp = wts.shape[1]
    n_tp = gains.shape[0]
    z, y, x, c = sp // 2, sp % 2, tp // 2, tp % 2
    leader = z % 2
    lead = c == leader
    keep = c != leader
    home = (z // 2 * 2 + 1 - c) * 2 + y
    rows, rank = raw_lat.shape
    quarter = rows // n_tp
    weights = (up_gate, up_value, down_weight)
    depth, ff = up_gate.shape
    width = n_sp * depth
    features = resid.shape[1]
    sib = (sp, x * 2 + 1 - c)
    xdev = (sp, (1 - x) * 2 + c)
    ydev = (z * 2 + 1 - y, tp)

    def zflip(a):
        return jnp.where(a == 1, z // 2 * 2 + 1 - z % 2, jnp.where(a == 2, (z + 2) % 4, 3 - z))

    def remote(src, dst, ss, rs, dev):
        return pltpu.make_async_remote_copy(
            src_ref=src, dst_ref=dst, send_sem=ss, recv_sem=rs, device_id=dev, device_id_type=MESH
        )

    barrier = pltpu.get_barrier_semaphore()
    for ds_ in range(n_sp):
        for dt in range(n_tp):
            if ds_ or dt:
                pl.semaphore_signal(
                    barrier,
                    inc=1,
                    device_id=(lax.rem(sp + ds_, n_sp), lax.rem(tp + dt, n_tp)),
                    device_id_type=MESH,
                )

    wide_cols = expand_wide.shape[1]
    loads = [
        (latent, raw_lat),
        (rope_key, raw_rope),
        (query_wide, raw_qw),
        (query_narrow, raw_qn),
        (expand_wide, expand.at[:, pl.ds(0, wide_cols)]),
        (expand_narrow, expand.at[:, pl.ds(wide_cols, expand_narrow.shape[1])]),
        (out_wide, outcat.at[pl.ds(0, out_wide.shape[0])]),
        (out_narrow, outcat.at[pl.ds(out_wide.shape[0], out_narrow.shape[0])]),
        (residual, resid),
    ]
    copies = [
        pltpu.make_async_copy(src, dst, local_sem.at[i]) for i, (src, dst) in enumerate(loads)
    ]
    for copy in copies:
        copy.start()

    lane = lax.broadcasted_iota(jnp.int32, (rows, LANES), 1)
    low = lane < ROPE
    copies[0].wait()
    copies[1].wait()
    base = coarse_tab[:, pl.ds(sp, 1), :]
    cosine = base[0] * fine_tab[0] - base[1] * fine_tab[1]
    sine = base[1] * fine_tab[0] + base[0] * fine_tab[1]
    sine = jnp.where(lane % ROPE < ROPE // 2, -sine, sine)

    def turn(values):
        return values * cosine + swap_halves(values, lane) * sine

    lat_f = raw_lat[...].astype(jnp.float32)
    square = jnp.mean(lat_f * lat_f, axis=-1, keepdims=True)
    lat_all[sp, :, 0:rank] = (lat_f * lax.rsqrt(square + epsilon) * latent_gain[...]).astype(
        jnp.bfloat16
    )
    rope_f = raw_rope[...].astype(jnp.float32)
    rope_f = jnp.concatenate([rope_f, rope_f], axis=1)
    lat_all[sp, :, rank:] = turn(rope_f).astype(jnp.bfloat16)

    with jax.named_scope("barw"):
        pl.semaphore_wait(barrier, n_sp * n_tp - 1)

    def piece(owner, who):
        return lat_all.at[owner, pl.ds(pl.multiple_of(who * quarter, quarter), quarter)]

    def z_copy(a):
        return remote(
            piece(sp, tp), piece(sp, tp), z_s.at[a - 1], own_r.at[a + 1], (zflip(a) * 2 + y, tp)
        )

    def owner_of(i):
        b = jnp.where((i == 1) | (i >= 5), 1, 0)
        a = jnp.where(i <= 1, 0, jnp.where(i <= 4, i - 1, i - 4))
        oz = jnp.where(a == 0, z, zflip(a))
        return oz * 2 + jnp.where(b == 1, 1 - y, y)

    def y_copy(i):
        own = piece(owner_of(i), tp)
        return remote(own, own, y_s.at[i], own_r.at[jnp.where(i == 0, 1, i + 3)], ydev)

    def sib_copy(i):
        own = piece(owner_of(i), tp)
        return remote(own, own, sib_s.at[i], sib_r.at[i], sib)

    def x_copy(i):
        own = piece(owner_of(i), tp)
        return remote(own, own, x_s.at[i], x_r.at[i], xdev)

    def xs_copy(i):
        other = piece(owner_of(i), (1 - x) * 2 + c)
        return remote(other, other, xs_s.at[i], xs_r.at[i], sib)

    def stage_one(i):
        y_arrival = piece(owner_of(i), tp)
        remote(y_arrival, y_arrival, y_s.at[0], own_r.at[i], sib).wait_recv()
        x_copy(i).start()
        sib_copy(i).start()

    def stage_two(i):
        x_copy(i).wait_recv()
        xs_copy(i).start()

    y_copy(0).start()
    for a in (1, 2, 3):
        z_copy(a).start()

    block = 2 * LANES
    cut = (ff // block + 1) // 2 * block
    half_depth = depth // 2
    col_parts = (pl.ds(0, cut), pl.ds(cut, ff - cut))
    row_parts = (pl.ds(0, half_depth), pl.ds(half_depth, half_depth))
    n_mix, n_all = 4, 6

    def chunk_src(q):
        if q < n_mix:
            return weights[q % 2].at[:, col_parts[q // 2]]
        return weights[2].at[row_parts[q - n_mix]]

    def chunk_dst(q, owner):
        if q < n_mix:
            return wts.at[q % 2, owner, :, col_parts[q // 2]]
        return wts.at[2, owner, row_parts[q - n_mix]]

    def z_weight(q, slot, a):
        return remote(
            chunk_src(q),
            chunk_dst(q, sp),
            wz_s.at[q, slot],
            wt_r.at[q, a + 1],
            (zflip(a) * 2 + y, tp),
        )

    def y_weight(q, k):
        own = isinstance(k, int) and k == 0
        here = chunk_dst(q, owner_of(k))
        return remote(
            chunk_src(q) if own else here,
            here,
            wy_s.at[q, k],
            wt_r.at[q, 1 if own else k + 3],
            ydev,
        )

    def sib_weight(q, k):
        own = isinstance(k, int) and k == 0
        here = chunk_dst(q, owner_of(k))
        return remote(chunk_src(q) if own else here, here, ws_s.at[q, k], wt_r.at[q, k], sib)

    def own_weight(q):
        return pltpu.make_async_copy(chunk_src(q), chunk_dst(q, sp), wt_r.at[q, 0])

    def wait_weight(q, k):
        ref = chunk_dst(q, owner_of(k))
        remote(ref, ref, wy_s.at[q, 0], wt_r.at[q, k], sib).wait_recv()

    def send_lead(q):
        z_weight(q, 0, 2).start()

    def send_other(first, last):
        for q in range(first, last):
            z_weight(q, 0, 1).start()
        for q in range(first, last):
            z_weight(q, 1, 3).start()

    @pl.when(lead)
    def _():
        for q in range(n_mix):
            send_lead(q)

    @pl.when(keep)
    def _():
        send_other(0, n_mix)

    gains[tp] = norm_gain[...]
    gain_peers = [(sp, lax.rem(tp + d, n_tp)) for d in range(1, n_tp)]

    def gain_copy(d):
        return remote(
            norm_gain, gains.at[tp], gain_s.at[d], gain_r.at[d], (sp, lax.rem(tp + d + 1, n_tp))
        )

    for d in range(n_tp - 1):
        gain_copy(d).start()

    def tap_copy():
        return remote(conv_taps, taps, tap_s.at[0], tap_r.at[0], sib)

    @pl.when(lead)
    def _():
        tap_copy().start()
        taps[...] = conv_taps[...]

    copies[2].wait()
    copies[3].wait()
    one = raw_qw[:, LANES : 2 * LANES].astype(jnp.float32)
    two = raw_qw[:, 2 * LANES :].astype(jnp.float32)
    turned_two = turn(two)
    qw[0, :, 0:LANES] = raw_qw[:, 0:LANES]
    qw[0, :, LANES:] = jnp.where(low, turn(one), 0.0).astype(jnp.bfloat16)
    qw[1, :, 0:LANES] = jnp.where(
        low, pltpu.roll(one, ROPE, 1), pltpu.roll(two, ROPE, 1)
    ).astype(jnp.bfloat16)
    qw[1, :, LANES:] = jnp.where(low, pltpu.roll(turned_two, ROPE, 1), 0.0).astype(jnp.bfloat16)
    for h in range(2):
        tile = raw_qn[:, h * LANES : (h + 1) * LANES].astype(jnp.float32)
        qn[h] = jnp.where(low, tile, turn(tile)).astype(jnp.bfloat16)
        vw[h, :, LANES:] = jnp.ones((rows, LANES), jnp.bfloat16)
    peak[...] = jnp.full(peak.shape, -1e30, jnp.float32)
    accw[...] = jnp.zeros(accw.shape, jnp.float32)
    accn[...] = jnp.zeros(accn.shape, jnp.float32)
    for i in (4, 5, 6, 7, 8):
        copies[i].wait()

    tile_rows = rows // 2

    def attend_tile(slot, query, key, value, acc, at, scale):
        scores = lax.dot_general(
            query, key, (((1,), (1,)), ((), ())), preferred_element_type=jnp.float32
        )
        before = peak[slot, at, :]
        after = jnp.maximum(before, jnp.max(scores, axis=-1, keepdims=True))
        pieces = [
            jnp.exp2((scores[:, j : j + LANES] - after) * scale)
            for j in range(0, scores.shape[1], LANES)
        ]
        spread = jnp.concatenate(pieces, axis=1).astype(jnp.bfloat16)
        keep = jnp.exp2((before - after) * scale)
        new = jnp.dot(spread, value, preferred_element_type=jnp.float32)
        for j in range(0, new.shape[1], LANES):
            acc[at, j : j + LANES] = acc[at, j : j + LANES] * keep + new[:, j : j + LANES]
        peak[slot, at, :] = after

    scale_w = (NOPE_W + ROPE) ** (-0.5) * math.log2(math.e)
    scale_n = (NOPE_N + ROPE) ** (-0.5) * math.log2(math.e)

    def block_step(i, carry):
        @pl.when(i == 1)
        @jax.named_scope("st0")
        def _():
            stage_one(i)
            stage_one(i + 1)
            stage_two(i)
            y_copy(i + 1).start()

        @pl.when((i >= 1) & (i <= 5))
        @jax.named_scope("st1")
        def _():
            stage_one(i + 2)

        @pl.when((i >= 1) & (i <= 2))
        def _():
            y_copy(i + 2).start()

        @pl.when((i >= 1) & (i <= 6))
        @jax.named_scope("st2")
        def _():
            stage_two(i + 1)

        @pl.when((i == 3) & lead)
        def _():
            for q in range(n_all):
                y_weight(q, 0).start()
                sib_weight(q, 0).start()
                own_weight(q).start()

        @pl.when(i >= 1)
        @jax.named_scope("stA")
        def _():
            sib_copy(i).wait_recv()
            xs_copy(i).wait_recv()

        owner = owner_of(i)
        shared = lat_all[owner, :, 0:rank]
        rope = lat_all[owner, :, rank:].astype(jnp.float32)
        for h in range(2):
            pair = jnp.dot(
                shared,
                expand[:, h * 2 * LANES : (h + 1) * 2 * LANES],
                preferred_element_type=jnp.float32,
            )
            kw[h, :, 0:LANES] = pair[:, 0:LANES].astype(jnp.bfloat16)
            kw[h, :, LANES:] = lat_all[owner, :, rank:]
            vw[h, :, 0:LANES] = pair[:, LANES:].astype(jnp.bfloat16)
        pair = jnp.dot(shared, expand[:, wide_cols:], preferred_element_type=jnp.float32)
        for h in range(2):
            mine = pair[:, h * LANES : (h + 1) * LANES]
            kn[h] = jnp.where(low, mine, rope).astype(jnp.bfloat16)
            vn[h] = jnp.where(low, 1.0, mine).astype(jnp.bfloat16)
        for t in range(rows // tile_rows):
            at = pl.ds(t * tile_rows, tile_rows)
            for h in range(2):
                attend_tile(h, qw[h, at, :], kw[h], vw[h], accw.at[h], at, scale_w)
                attend_tile(2 + h, qn[h, at, :], kn[h], vn[h], accn.at[h], at, scale_n)
        return carry

    lax.fori_loop(0, n_sp, block_step, 0)

    for h in range(2):
        heads[:, h * LANES : (h + 1) * LANES] = (
            accw[h, :, 0:LANES] / accw[h, :, LANES:]
        ).astype(jnp.bfloat16)
    first, second = accn[0], accn[1]
    first_r, second_r = pltpu.roll(first, ROPE, 1), pltpu.roll(second, ROPE, 1)
    heads[:, 2 * LANES :] = (
        jnp.where(low, first_r, second) / jnp.where(low, first, second_r)
    ).astype(jnp.bfloat16)

    step_rows = LANES
    n_steps = rows // step_rows

    def tile_at(t):
        return pl.ds(pl.multiple_of(t * step_rows, step_rows), step_rows)

    def part_copy(t):
        return remote(
            xsend.at[tile_at(t)], part_in.at[tile_at(t)], part_s.at[t], part_r.at[t], sib
        )

    def bx_copy(t):
        return remote(xsend.at[tile_at(t)], xrecv.at[tile_at(t)], bx_s.at[t], bx_r.at[t], xdev)

    pair_dev = (zflip(1) * 2 + y, tp)

    x_cols = n_tp // 2 * features

    def swap_copy(t):
        part = att.at[tile_at(t), pl.ds(pl.multiple_of(x * x_cols, x_cols), x_cols)]
        return remote(part, part, swap_s.at[t], swap_r.at[t], pair_dev)

    def cross_copy(t):
        part = att.at[tile_at(t), pl.ds(pl.multiple_of(x * x_cols, x_cols), x_cols)]
        return remote(part, part, cross_s.at[t], cross_r.at[t], xdev)

    @jax.named_scope("proj")
    def project(t, carry):
        at = tile_at(t)
        pieces = []
        for j in range(n_tp):
            cols = slice(j * features, (j + 1) * features)
            term = jnp.dot(heads[at, :], outcat[:, cols], preferred_element_type=jnp.float32)
            mine = jnp.where(tp == j, 1.0, 0.0)
            pieces.append(term + resid[at, :].astype(jnp.float32) * mine)

        @pl.when(lead)
        def _():
            for j in range(n_tp):
                cols = slice(j * features, (j + 1) * features)
                xsend[at, cols] = pieces[j].astype(jnp.bfloat16)
            part_copy(t).start()

        @pl.when(keep)
        def _():
            part_copy(t).wait_recv()
            for j in range(n_tp):
                cols = slice(j * features, (j + 1) * features)
                xsend[at, cols] = (
                    pieces[j] + part_in[at, cols].astype(jnp.float32)
                ).astype(jnp.bfloat16)
            bx_copy(t).start()

        return carry

    lax.fori_loop(0, n_steps, project, 0)

    def forward_z(q):
        with jax.named_scope(f"fz{q}"):
            for k in (2, 3, 4):
                wait_weight(q, k)
                y_weight(q, k).start()
                sib_weight(q, k).start()

    def forward_far(q):
        with jax.named_scope(f"fz{q}"):
            for k in (3, 4, 2):
                wait_weight(q, k)
                y_weight(q, k).start()
                sib_weight(q, k).start()

    def forward_y(q):
        with jax.named_scope(f"fy{q}"):
            for k in (1, 5, 6, 7):
                wait_weight(q, k)
                sib_weight(q, k).start()

    def halo_copy(side, plane):
        there = sp - 1 if side == 1 else sp + 1
        tz, ty = there // 2, there % 2
        src = att.at[pl.ds(0, HALO)] if side == 1 else att.at[pl.ds(rows - HALO, HALO)]
        dev = ((tz // 2 * 2 + plane) * 2 + ty, x * 2 + 1 - tz % 2)
        return remote(src, halo.at[side], halo_s.at[side, plane], halo_r.at[side], dev)

    def attq_copy(col):
        return remote(
            att.at[:, pl.ds(pl.multiple_of(col * features, features), features)],
            att_q,
            attq_s.at[0],
            attq_r.at[0],
            sib,
        )

    @jax.named_scope("exch")
    def exchange(t):
        at = tile_at(t)
        bx_copy(t).wait_recv()
        att[at, :] = (
            xsend[at, :].astype(jnp.float32) + xrecv[at, :].astype(jnp.float32)
        ).astype(jnp.bfloat16)
        swap_copy(t).start()

    def on_lead(*steps):
        @pl.when(lead)
        def _():
            for step, arg in steps:
                step(arg)

    def send_late(q):
        for q in range(n_mix, n_all):
            send_lead(q)

    @jax.named_scope("swapw")
    def swap_wait(q):
        for t in range(n_steps):
            swap_copy(t).wait_recv()
            cross_copy(t).start()

    @jax.named_scope("crossw")
    def cross_wait(q):
        for t in range(n_steps):
            cross_copy(t).wait_recv()

    on_lead(
        (forward_z, 0),
        (forward_z, 1),
        (forward_y, 0),
        (forward_z, 2),
        (forward_y, 1),
        (forward_z, 3),
        (send_late, 0),
        (swap_wait, 0),
        (forward_y, 2),
        (cross_wait, 0),
    )

    @pl.when(keep)
    def _():
        for t in range(n_steps):
            exchange(t)

        @pl.when(sp > 0)
        def _():
            for plane in range(2):
                halo_copy(1, plane).start()

        @pl.when(sp < n_sp - 1)
        def _():
            for plane in range(2):
                halo_copy(0, plane).start()

        attq_copy(x * 2 + 1 - c).start()
        for q in range(n_mix, n_all):
            z_weight(q, 1, 3).start()
        for q in range(n_mix, n_all):
            z_weight(q, 0, 1).start()
        att_q[...] = att[:, pl.ds(pl.multiple_of(tp * features, features), features)]

    for d in range(n_tp - 1):
        gain_copy(d).wait_recv()

    def normalize(values):
        values = values.astype(jnp.float32)
        factor = lax.rsqrt(jnp.mean(values * values, axis=-1, keepdims=True) + epsilon)
        return jnp.concatenate(
            [
                values[:, j * features : (j + 1) * features] * factor * gains[j]
                for j in range(n_tp)
            ],
            axis=1,
        )

    def norm_step(t, carry):
        normed[tile_at(t), :] = normalize(att[tile_at(t), :]).astype(jnp.bfloat16)
        return carry

    lax.fori_loop(0, n_steps, norm_step, 0)

    def halo_wait(side):
        remote(
            halo.at[side], halo.at[side], halo_s.at[side, 0], halo_r.at[side], sib
        ).wait_recv()

    @pl.when(home > 0)
    @jax.named_scope("halo0")
    def _():
        halo_wait(0)

    @pl.when(home < n_sp - 1)
    @jax.named_scope("halo1")
    def _():
        halo_wait(1)

    previous = jnp.where(home > 0, normalize(halo[0])[HALO - 1 :, :], 0.0)
    following = jnp.where(home < n_sp - 1, normalize(halo[1])[0:1, :], 0.0)
    edge = lax.broadcasted_iota(jnp.int32, (HALO, width), 0)
    normed[rows:, :] = jnp.where(
        edge == 0, previous, jnp.where(edge == 1, following, 0.0)
    ).astype(jnp.bfloat16)

    def ready(part):
        for q in (2 * part, 2 * part + 1):
            own_weight(q).wait()

    def arrived(part):
        with jax.named_scope(f"arr{part}"):
            for q in (2 * part, 2 * part + 1):
                for k in range(n_sp):
                    wait_weight(q, k)

    on_lead((ready, 0))

    @pl.when(keep)
    def _():
        tap_copy().wait_recv()
        arrived(0)

    def smooth(values, cols, which):
        size = values.shape[1]
        row = lax.broadcasted_iota(jnp.int32, (rows, size), 0)
        values = values.astype(jnp.bfloat16).astype(jnp.float32)
        main = values[0:rows]
        before = jnp.where(row == 0, values[rows : rows + 1], pltpu.roll(main, 1, 0))
        after = jnp.where(
            row == rows - 1, values[rows + 1 : rows + 2], pltpu.roll(main, rows - 1, 0)
        )
        return (
            taps[0, which : which + 1, cols] * before
            + taps[1, which : which + 1, cols] * main
            + taps[2, which : which + 1, cols] * after
        )

    def mix(start, size):
        cols = pl.ds(start, size)
        both = []
        for m in range(2):
            rhs = wts[m, :, :, cols].reshape(width, size)
            both.append(
                smooth(jnp.dot(normed[...], rhs, preferred_element_type=jnp.float32), cols, m)
            )
        gate = both[0]
        hidden[:, cols] = (gate / (1.0 + jnp.exp(-gate)) * both[1]).astype(jnp.bfloat16)

    @jax.named_scope("mix")
    def mix_step(j, carry):
        mix(pl.multiple_of(j * block, block), block)
        return carry

    early = cut // block - 1
    lax.fori_loop(0, early, mix_step, 0)
    on_lead((forward_y, 3), (ready, 1))
    lax.fori_loop(early, cut // block, mix_step, 0)

    @pl.when(keep)
    def _():
        arrived(1)

    lax.fori_loop(cut // block, ff // block, mix_step, 0)
    if ff % block:
        mix(ff // block * block, ff % block)

    parts = features // depth
    per_x = n_sp // 2
    source = jnp.where(home == sp, 0, 1)

    def ours(owner):
        return owner // per_x == x

    def ox_copy(i, owner):
        return remote(
            osend.at[i], orx.at[owner % per_x], ox_s.at[i], ox_r.at[owner % per_x], xdev
        )

    def out_slot(owner):
        half = owner % parts
        return source, slice(None), pl.ds(pl.multiple_of(half * depth, depth), depth)

    def out_copy(i, owner):
        return remote(
            osend.at[i],
            orecv.at[out_slot(owner)],
            out_s.at[i],
            out_r.at[source, owner % parts],
            (home, owner // parts),
        )

    def mine(owner):
        return (home == sp) & (owner // parts == tp)

    def order(step):
        far = (step >= 2) & (step != 5) & (step != 4) & (step != 7)
        near = (step == 4) | (step == 7)
        return jnp.where(far, step + 1, jnp.where(near, step - 2, jnp.where(step == 5, 6, step)))

    @jax.named_scope("comb")
    def combine(step):
        i = order(step)
        owner = owner_of(i)

        @pl.when(ours(owner))
        def _():
            ox_copy(i, owner).wait_recv()
            both = (
                osend[i].astype(jnp.float32) + orx[owner % per_x].astype(jnp.float32)
            ).astype(jnp.bfloat16)

            @pl.when(mine(owner))
            def _():
                orecv[out_slot(owner)] = both

            @pl.when(jnp.logical_not(mine(owner)))
            def _():
                osend[i] = both
                out_copy(i, owner).start()

    lag = 3

    @jax.named_scope("down")
    def down_step(step, carry):
        i = order(step)

        @pl.when(lead & ((i == 1) | (i >= 5)))
        def _():
            for q in range(n_mix, n_all):
                wait_weight(q, i)
                sib_weight(q, i).start()

        @pl.when(lead & (i == 0))
        def _():
            for q in range(n_mix, n_all):
                own_weight(q).wait()

        @pl.when(keep)
        def _():
            for q in range(n_mix, n_all):
                wait_weight(q, i)

        owner = owner_of(i)
        osend[i] = lax.dot_general(
            hidden[...],
            wts[2, owner],
            (((1,), (1,)), ((), ())),
            preferred_element_type=jnp.float32,
        ).astype(jnp.bfloat16)

        @pl.when(jnp.logical_not(ours(owner)))
        def _():
            ox_copy(i, owner).start()

        @pl.when(step >= lag)
        def _():
            combine(step - lag)

        return carry

    lax.fori_loop(0, 2, down_step, 0)
    on_lead(*((forward_far, q) for q in range(n_mix, n_all)))
    lax.fori_loop(2, n_sp, down_step, 0)

    def last_step(i, carry):
        combine(i)
        return carry

    lax.fori_loop(n_sp - lag, n_sp, last_step, 0)

    @pl.when(lead)
    def _():
        attq_copy(0).wait_recv()

    for s in range(orecv.shape[0]):

        @pl.when(lead | (s == 1))
        @jax.named_scope("owait")
        def _():
            for half in range(parts):
                ref = orecv.at[s, :, pl.ds(half * depth, depth)]
                remote(ref, ref, out_s.at[0], out_r.at[s, half], sib).wait_recv()

    total = att_q[...].astype(jnp.float32)
    for s in range(orecv.shape[0]):
        total = total + orecv[s].astype(jnp.float32)
    result[...] = total.astype(jnp.bfloat16)
    store = pltpu.make_async_copy(result, output, local_sem.at[0])
    store.start()

    y_copy(0).wait_send()
    for i in (2, 3, 4):
        y_copy(i).wait_send()
    for a in (1, 2, 3):
        z_copy(a).wait_send()
    for i in range(1, n_sp):
        x_copy(i).wait_send()
        sib_copy(i).wait_send()
        xs_copy(i).wait_send()
    for d in range(n_tp - 1):
        gain_copy(d).wait_send()

    @pl.when(lead)
    def _():
        tap_copy().wait_send()
        for q in range(n_all):
            z_weight(q, 0, 2).wait_send()
            for k in (0, 2, 3, 4):
                y_weight(q, k).wait_send()
            for k in range(n_sp):
                sib_weight(q, k).wait_send()
        for t in range(n_steps):
            part_copy(t).wait_send()
            cross_copy(t).wait_send()

    @pl.when(keep)
    def _():
        attq_copy(0).wait_send()
        for q in range(n_all):
            z_weight(q, 0, 1).wait_send()
            z_weight(q, 1, 3).wait_send()
        for t in range(n_steps):
            bx_copy(t).wait_send()
            swap_copy(t).wait_send()

        @pl.when(sp > 0)
        def _():
            for plane in range(2):
                halo_copy(1, plane).wait_send()

        @pl.when(sp < n_sp - 1)
        def _():
            for plane in range(2):
                halo_copy(0, plane).wait_send()

    def out_wait(i, carry):
        owner = owner_of(i)

        @pl.when(jnp.logical_not(ours(owner)))
        def _():
            ox_copy(i, owner).wait_send()

        @pl.when(ours(owner) & jnp.logical_not(mine(owner)))
        def _():
            out_copy(i, owner).wait_send()

        return carry

    lax.fori_loop(0, n_sp, out_wait, 0)
    store.wait()


def fused_device(n_sp, n_tp, *arrays):
    (
        residual,
        query_wide,
        query_narrow,
        latent,
        rope_key,
        latent_gain,
        expand_wide,
        expand_narrow,
        out_wide,
        out_narrow,
        norm_gain,
        up_gate,
        up_value,
        down_weight,
        conv_taps,
    ) = arrays
    rows, features = residual.shape
    rank = latent.shape[1]
    depth, ff = up_gate.shape
    width = n_sp * depth
    fine, coarse = turn_tables(rows, n_sp)
    operands = (
        residual,
        query_wide,
        query_narrow,
        latent,
        rope_key,
        latent_gain[None],
        expand_wide,
        expand_narrow,
        out_wide,
        out_narrow,
        norm_gain[None],
        up_gate,
        up_value,
        down_weight,
        conv_taps,
        jnp.asarray(fine),
        jnp.asarray(coarse),
    )
    small = (5, 10, 14, 15, 16)
    anywhere = pl.BlockSpec(memory_space=pl.ANY)
    inside = pl.BlockSpec(memory_space=pltpu.VMEM)
    low, full = jnp.bfloat16, jnp.float32
    buffers = [
        ((n_sp, rows, rank + LANES), low),
        ((3, n_sp, depth, ff), low),
        ((rows, rank), low),
        ((rows, ROPE), low),
        (query_wide.shape, low),
        (query_narrow.shape, low),
        ((2, rows, 2 * LANES), low),
        ((2, rows, LANES), low),
        ((2, rows, 2 * LANES), low),
        ((2, rows, 2 * LANES), low),
        ((2, rows, LANES), low),
        ((2, rows, LANES), low),
        ((2, rows, 2 * LANES), full),
        ((2, rows, LANES), full),
        ((4, rows, LANES), full),
        ((rank, expand_wide.shape[1] + expand_narrow.shape[1]), low),
        ((out_wide.shape[0] + out_narrow.shape[0], width), low),
        ((rows, features), low),
        ((rows, out_wide.shape[0] + out_narrow.shape[0]), low),
        ((rows, width), low),
        ((rows, width), low),
        ((rows, width), low),
        ((rows, width), low),
        ((rows, features), low),
        ((rows + HALO, width), low),
        ((2, HALO, width), low),
        ((n_tp, 1, features), full),
        (conv_taps.shape, full),
        ((rows, ff), low),
        ((n_sp, rows, depth), low),
        ((n_sp // 2, rows, depth), low),
        ((2, rows, features), low),
        ((rows, features), low),
    ]
    steps = rows // LANES
    semaphores = [
        (9,),
        (8,),
        (8,),
        (8,),
        (8,),
        (3,),
        (5,),
        (8,),
        (8,),
        (8,),
        (6, 8),
        (6, 2),
        (6, 5),
        (6, 8),
        (steps,),
        (steps,),
        (steps,),
        (steps,),
        (steps,),
        (steps,),
        (steps,),
        (steps,),
        (2,),
        (2, 2),
        (1,),
        (1,),
        (3,),
        (3,),
        (1,),
        (1,),
        (4,),
        (8,),
        (2, features // depth),
        (8,),
    ]
    return pl.pallas_call(
        fused_kernel,
        out_shape=jax.ShapeDtypeStruct((rows, features), jnp.bfloat16),
        in_specs=[inside if i in small else anywhere for i in range(len(operands))],
        out_specs=anywhere,
        scratch_shapes=[pltpu.VMEM(shape, dtype) for shape, dtype in buffers]
        + [pltpu.SemaphoreType.DMA(shape) for shape in semaphores],
        compiler_params=pltpu.CompilerParams(
            collective_id=0, has_side_effects=True, vmem_limit_bytes=67043328
        ),
    )(*operands)


def solution(mesh):
    in_specs = (
        P("sp", "tp"),
        P("sp", "tp"),
        P("sp", "tp"),
        P("sp", None),
        P("sp", None),
        P(),
        P(None, "tp"),
        P(None, "tp"),
        P("tp", None),
        P("tp", None),
        P("tp"),
        P("sp", "tp"),
        P("sp", "tp"),
        P("sp", "tp"),
        P(None, None, "tp"),
    )
    out_specs = P("sp", "tp")
    n_sp, n_tp = mesh.shape["sp"], mesh.shape["tp"]
    body = per_device
    if (n_sp, n_tp) == (8, 4):
        body = functools.partial(fused_device, n_sp, n_tp)
    return jax.shard_map(
        body, mesh=mesh, in_specs=in_specs, out_specs=out_specs, check_vma=False
    )
```

```python
import functools
import math

import jax
import jax.numpy as jnp
import numpy as np
from jax import lax
from jax.experimental import pallas as pl
from jax.experimental.pallas import tpu as pltpu
from jax.sharding import PartitionSpec as P

D = 2048
ROPE = 64
NOPE_W = 128
VAL_W = 128
NOPE_N = 64
VAL_N = 64


theta = 10000.0
epsilon = 1e-06


def padded(block, sides, width):
    for axis, dim in sides:
        count = lax.axis_size(axis)
        forward = [(i, i + 1) for i in range(count - 1)]
        backward = [(target, source) for source, target in forward]
        low = lax.ppermute(
            lax.slice_in_dim(block, block.shape[dim] - width, None, axis=dim), axis, forward
        )
        high = lax.ppermute(lax.slice_in_dim(block, 0, width, axis=dim), axis, backward)
        block = jnp.concatenate([low, block, high], axis=dim)
    return block


def rotate(values, positions):
    half_dim = values.shape[-1] // 2
    inverse = jnp.power(
        jnp.float32(theta), -2.0 * jnp.arange(half_dim, dtype=jnp.float32) / values.shape[-1]
    )
    angles = positions[:, None] * inverse[None, :]
    new_shape = (angles.shape[0],) + (1,) * (values.ndim - 2) + (half_dim,)
    cosine = jnp.cos(angles).reshape(new_shape)
    sine_part = jnp.sin(angles).reshape(new_shape)
    floats = values.astype(jnp.float32)
    lower_half = floats[..., :half_dim]
    upper_half = floats[..., half_dim:]
    turned = jnp.concatenate(
        [
            lower_half * cosine - upper_half * sine_part,
            lower_half * sine_part + upper_half * cosine,
        ],
        axis=-1,
    )
    return turned.astype(jnp.bfloat16)


def turn_query(queries, head_count, nope_dim, positions):
    shaped = queries.reshape(queries.shape[0], head_count, nope_dim + ROPE)
    return jnp.concatenate(
        [shaped[..., :nope_dim], rotate(shaped[..., nope_dim:], positions)], axis=-1
    )


def attend_kernel(scale, chunk, q_ref, k_ref, v_ref, o_ref):
    query = q_ref[0]
    rows = query.shape[0]
    value_dim = v_ref.shape[-1]
    row_max = jnp.full((rows, 1), -1e30, jnp.float32)
    row_total = jnp.zeros((rows, 1), jnp.float32)
    weighted = jnp.zeros((rows, value_dim), jnp.float32)
    for start in range(0, k_ref.shape[1], chunk):
        scores = lax.dot_general(
            query,
            k_ref[0, start : start + chunk, :],
            (((1,), (1,)), ((), ())),
            preferred_element_type=jnp.float32,
        )
        new_max = jnp.maximum(row_max, jnp.max(scores, axis=-1, keepdims=True))
        weights = jnp.exp2((scores - new_max) * scale)
        keep = jnp.exp2((row_max - new_max) * scale)
        row_total = row_total * keep + jnp.sum(weights, axis=-1, keepdims=True)
        weighted = weighted * keep + jnp.dot(
            weights.astype(jnp.bfloat16),
            v_ref[0, start : start + chunk, :],
            preferred_element_type=jnp.float32,
        )
        row_max = new_max
    o_ref[0] = (weighted / row_total).astype(o_ref.dtype)


def attend(query, key, value, factor):
    heads, rows, width = query.shape
    count = key.shape[1]
    value_dim = value.shape[-1]
    block = math.gcd(rows, 320)
    chunk = math.gcd(count, 1024)
    return pl.pallas_call(
        functools.partial(attend_kernel, factor * math.log2(math.e), chunk),
        grid=(heads, rows // block),
        in_specs=[
            pl.BlockSpec((1, block, width), lambda h, i: (h, i, 0)),
            pl.BlockSpec((1, count, width), lambda h, i: (h, 0, 0)),
            pl.BlockSpec((1, count, value_dim), lambda h, i: (h, 0, 0)),
        ],
        out_specs=pl.BlockSpec((1, block, value_dim), lambda h, i: (h, i, 0)),
        out_shape=jax.ShapeDtypeStruct((heads, rows, value_dim), jnp.bfloat16),
        compiler_params=pltpu.CompilerParams(
            dimension_semantics=("arbitrary", "arbitrary"), vmem_limit_bytes=48 << 20
        ),
        cost_estimate=pl.CostEstimate(
            flops=2 * heads * rows * count * 512,
            bytes_accessed=2 * heads * count * (width + value_dim),
            transcendentals=heads * rows * count,
        ),
    )(query, key, value)


def key_value(latent, expand, head_count, key_dim, rope):
    pair = expand.reshape(expand.shape[0], head_count, -1)
    key = jnp.einsum(
        "td,dhn->htn", latent, pair[..., :key_dim], preferred_element_type=jnp.float32
    ).astype(jnp.bfloat16)
    value = jnp.einsum(
        "td,dhn->htn", latent, pair[..., key_dim:], preferred_element_type=jnp.float32
    ).astype(jnp.bfloat16)
    shared = jnp.broadcast_to(rope[None], (head_count,) + rope.shape)
    return jnp.concatenate([key, shared], axis=-1), value


def side_by_side(heads):
    return jnp.transpose(heads, (1, 0, 2)).reshape(heads.shape[1], -1)


def per_device(
    residual,
    query_wide,
    query_narrow,
    latent,
    rope_key,
    latent_gain,
    expand_wide,
    expand_narrow,
    out_wide,
    out_narrow,
    norm_gain,
    up_gate,
    up_value,
    down_weight,
    conv_taps,
):
    tok_rows = residual.shape[0]
    offset = lax.axis_index("sp") * tok_rows
    positions = (offset + lax.iota(jnp.int32, tok_rows)).astype(jnp.float32)
    latent_float = latent.astype(jnp.float32)
    normed_latent = (
        latent_float
        * lax.rsqrt(jnp.mean(latent_float * latent_float, axis=-1, keepdims=True) + epsilon)
        * latent_gain
    ).astype(jnp.bfloat16)
    rope_turned = rotate(rope_key, positions)
    wide_heads = query_wide.shape[1] // (NOPE_W + ROPE)
    narrow_heads = query_narrow.shape[1] // (NOPE_N + ROPE)
    query_w = turn_query(query_wide, wide_heads, NOPE_W, positions)
    query_n = turn_query(query_narrow, narrow_heads, NOPE_N, positions)
    gathered = lax.all_gather(
        jnp.concatenate([normed_latent, rope_turned, jnp.zeros_like(rope_turned)], axis=1),
        "sp",
        axis=0,
        tiled=True,
    )
    full_gain = lax.all_gather(norm_gain, "tp", axis=0, tiled=True)
    gathered, up_gate, up_value, down_weight = lax.optimization_barrier(
        (gathered, up_gate, up_value, down_weight)
    )
    gate_full, value_full, down_full = (
        lax.all_gather(up_gate, "sp", axis=0, tiled=True),
        lax.all_gather(up_value, "sp", axis=0, tiled=True),
        lax.all_gather(down_weight, "sp", axis=0, tiled=True),
    )
    rank = latent.shape[1]
    latent_all, rope_all = gathered[:, :rank], gathered[:, rank : rank + ROPE]
    key_w, value_w = key_value(latent_all, expand_wide, wide_heads, NOPE_W, rope_all)
    key_n, value_n = key_value(latent_all, expand_narrow, narrow_heads, NOPE_N, rope_all)
    heads_wide = side_by_side(
        attend(jnp.transpose(query_w, (1, 0, 2)), key_w, value_w, (NOPE_W + ROPE) ** (-0.5))
    )
    heads_narrow = side_by_side(
        attend(jnp.transpose(query_n, (1, 0, 2)), key_n, value_n, (NOPE_N + ROPE) ** (-0.5))
    )
    head_terms = jnp.dot(heads_wide, out_wide, preferred_element_type=jnp.float32)
    head_terms = head_terms + jnp.dot(heads_narrow, out_narrow, preferred_element_type=jnp.float32)
    head_terms, gate_full, value_full = lax.optimization_barrier(
        (head_terms.astype(jnp.bfloat16), gate_full, value_full)
    )
    head_shares = lax.psum_scatter(
        head_terms, "tp", scatter_dimension=1, tiled=True
    ).astype(jnp.float32)
    attended = (residual.astype(jnp.float32) + head_shares).astype(jnp.bfloat16)
    attended_float = attended.astype(jnp.float32)
    attended_full = lax.all_gather(attended, "tp", axis=1, tiled=True).astype(jnp.float32)
    squares = jnp.mean(attended_full * attended_full, axis=-1, keepdims=True)
    normed_full = (attended_full * lax.rsqrt(squares + epsilon) * full_gain).astype(jnp.bfloat16)
    gate_float = jnp.dot(normed_full, gate_full, preferred_element_type=jnp.float32)
    value_float = jnp.dot(normed_full, value_full, preferred_element_type=jnp.float32)
    gate_width = up_gate.shape[1]
    both_up = jnp.concatenate(
        [gate_float.astype(jnp.bfloat16), value_float.astype(jnp.bfloat16)], axis=1
    )
    extended = padded(both_up, (("sp", 0),), 1).astype(jnp.float32)
    tap_rows = conv_taps.reshape(3, 2 * gate_width)
    smoothed = (
        tap_rows[0] * extended[:-2] + tap_rows[1] * extended[1:-1] + tap_rows[2] * extended[2:]
    )
    hidden = (jax.nn.silu(smoothed[:, :gate_width]) * smoothed[:, gate_width:]).astype(jnp.bfloat16)
    unit_terms = lax.dot_general(
        hidden, down_full, (((1,), (1,)), ((), ())), preferred_element_type=jnp.float32
    )
    unit_shares = lax.psum_scatter(
        unit_terms.astype(jnp.bfloat16), "tp", scatter_dimension=1, tiled=True
    ).astype(jnp.float32)
    return (attended_float + unit_shares).astype(jnp.bfloat16)


MESH = pl.DeviceIdType.MESH
LANES = 128
HALO = 16


def turn_tables(rows, groups):
    half = ROPE // 2
    inverse = np.power(theta, -2.0 * np.arange(half) / ROPE)
    inverse = np.tile(inverse, LANES // half)[None, :]
    local = np.arange(rows)[:, None] * inverse
    start = (np.arange(groups) * rows)[:, None] * inverse
    fine = np.stack([np.cos(local), np.sin(local)]).astype(np.float32)
    coarse = np.stack([np.cos(start), np.sin(start)]).astype(np.float32)
    return fine, coarse


def swap_halves(values, lane):
    half = ROPE // 2
    left = pltpu.roll(values, LANES - half, 1)
    right = pltpu.roll(values, half, 1)
    return jnp.where(lane % ROPE < half, left, right)


def fused_kernel(
    residual,
    query_wide,
    query_narrow,
    latent,
    rope_key,
    latent_gain,
    expand_wide,
    expand_narrow,
    out_wide,
    out_narrow,
    norm_gain,
    up_gate,
    up_value,
    down_weight,
    conv_taps,
    fine_tab,
    coarse_tab,
    output,
    lat_all,
    wts,
    raw_lat,
    raw_rope,
    raw_qw,
    raw_qn,
    qw,
    qn,
    kw,
    vw,
    kn,
    vn,
    accw,
    accn,
    peak,
    expand,
    outcat,
    resid,
    heads,
    part_in,
    xsend,
    xrecv,
    att,
    att_q,
    normed,
    halo,
    gains,
    taps,
    hidden,
    osend,
    orecv,
    result,
    local_sem,
    own_r,
    sib_r,
    x_r,
    xs_r,
    z_s,
    y_s,
    sib_s,
    x_s,
    xs_s,
    wt_r,
    wz_s,
    wy_s,
    ws_s,
    part_r,
    part_s,
    bx_r,
    bx_s,
    swap_r,
    swap_s,
    cross_r,
    cross_s,
    halo_r,
    halo_s,
    attq_r,
    attq_s,
    gain_r,
    gain_s,
    tap_r,
    tap_s,
    out_r,
    out_s,
):
    sp = lax.axis_index("sp")
    tp = lax.axis_index("tp")
    n_sp = wts.shape[1]
    n_tp = gains.shape[0]
    z, y, x, c = sp // 2, sp % 2, tp // 2, tp % 2
    leader = z % 2
    lead = c == leader
    keep = c != leader
    home = (z // 2 * 2 + 1 - c) * 2 + y
    rows, rank = raw_lat.shape
    quarter = rows // n_tp
    weights = (up_gate, up_value, down_weight)
    depth, ff = up_gate.shape
    width = n_sp * depth
    features = resid.shape[1]
    sib = (sp, x * 2 + 1 - c)
    xdev = (sp, (1 - x) * 2 + c)
    ydev = (z * 2 + 1 - y, tp)

    def zflip(a):
        return jnp.where(a == 1, z // 2 * 2 + 1 - z % 2, jnp.where(a == 2, (z + 2) % 4, 3 - z))

    def remote(src, dst, ss, rs, dev):
        return pltpu.make_async_remote_copy(
            src_ref=src, dst_ref=dst, send_sem=ss, recv_sem=rs, device_id=dev, device_id_type=MESH
        )

    barrier = pltpu.get_barrier_semaphore()
    for ds_ in range(n_sp):
        for dt in range(n_tp):
            if ds_ or dt:
                pl.semaphore_signal(
                    barrier,
                    inc=1,
                    device_id=(lax.rem(sp + ds_, n_sp), lax.rem(tp + dt, n_tp)),
                    device_id_type=MESH,
                )

    wide_cols = expand_wide.shape[1]
    loads = [
        (latent, raw_lat),
        (rope_key, raw_rope),
        (query_wide, raw_qw),
        (query_narrow, raw_qn),
        (expand_wide, expand.at[:, pl.ds(0, wide_cols)]),
        (expand_narrow, expand.at[:, pl.ds(wide_cols, expand_narrow.shape[1])]),
        (out_wide, outcat.at[pl.ds(0, out_wide.shape[0])]),
        (out_narrow, outcat.at[pl.ds(out_wide.shape[0], out_narrow.shape[0])]),
        (residual, resid),
    ]
    copies = [
        pltpu.make_async_copy(src, dst, local_sem.at[i]) for i, (src, dst) in enumerate(loads)
    ]
    for copy in copies:
        copy.start()

    lane = lax.broadcasted_iota(jnp.int32, (rows, LANES), 1)
    low = lane < ROPE
    copies[0].wait()
    copies[1].wait()
    base = coarse_tab[:, pl.ds(sp, 1), :]
    cosine = base[0] * fine_tab[0] - base[1] * fine_tab[1]
    sine = base[1] * fine_tab[0] + base[0] * fine_tab[1]
    sine = jnp.where(lane % ROPE < ROPE // 2, -sine, sine)

    def turn(values):
        return values * cosine + swap_halves(values, lane) * sine

    lat_f = raw_lat[...].astype(jnp.float32)
    square = jnp.mean(lat_f * lat_f, axis=-1, keepdims=True)
    lat_all[sp, :, 0:rank] = (lat_f * lax.rsqrt(square + epsilon) * latent_gain[...]).astype(
        jnp.bfloat16
    )
    rope_f = raw_rope[...].astype(jnp.float32)
    rope_f = jnp.concatenate([rope_f, rope_f], axis=1)
    lat_all[sp, :, rank:] = turn(rope_f).astype(jnp.bfloat16)

    with jax.named_scope("barw"):
        pl.semaphore_wait(barrier, n_sp * n_tp - 1)

    def piece(owner, who):
        return lat_all.at[owner, pl.ds(pl.multiple_of(who * quarter, quarter), quarter)]

    def z_copy(a):
        return remote(
            piece(sp, tp), piece(sp, tp), z_s.at[a - 1], own_r.at[a + 1], (zflip(a) * 2 + y, tp)
        )

    def owner_of(i):
        b = jnp.where((i == 1) | (i >= 5), 1, 0)
        a = jnp.where(i <= 1, 0, jnp.where(i <= 4, i - 1, i - 4))
        oz = jnp.where(a == 0, z, zflip(a))
        return oz * 2 + jnp.where(b == 1, 1 - y, y)

    def y_copy(i):
        own = piece(owner_of(i), tp)
        return remote(own, own, y_s.at[i], own_r.at[jnp.where(i == 0, 1, i + 3)], ydev)

    def sib_copy(i):
        own = piece(owner_of(i), tp)
        return remote(own, own, sib_s.at[i], sib_r.at[i], sib)

    def x_copy(i):
        own = piece(owner_of(i), tp)
        return remote(own, own, x_s.at[i], x_r.at[i], xdev)

    def xs_copy(i):
        other = piece(owner_of(i), (1 - x) * 2 + c)
        return remote(other, other, xs_s.at[i], xs_r.at[i], sib)

    def stage_one(i):
        y_arrival = piece(owner_of(i), tp)
        remote(y_arrival, y_arrival, y_s.at[0], own_r.at[i], sib).wait_recv()
        x_copy(i).start()
        sib_copy(i).start()

    def stage_two(i):
        x_copy(i).wait_recv()
        xs_copy(i).start()

    y_copy(0).start()
    for a in (1, 2, 3):
        z_copy(a).start()

    block = 2 * LANES
    cut = (ff // block + 1) // 2 * block
    half_depth = depth // 2
    col_parts = (pl.ds(0, cut), pl.ds(cut, ff - cut))
    row_parts = (pl.ds(0, half_depth), pl.ds(half_depth, half_depth))
    n_mix, n_all = 4, 6

    def chunk_src(q):
        if q < n_mix:
            return weights[q % 2].at[:, col_parts[q // 2]]
        return weights[2].at[row_parts[q - n_mix]]

    def chunk_dst(q, owner):
        if q < n_mix:
            return wts.at[q % 2, owner, :, col_parts[q // 2]]
        return wts.at[2, owner, row_parts[q - n_mix]]

    def z_weight(q, slot, a):
        return remote(
            chunk_src(q),
            chunk_dst(q, sp),
            wz_s.at[q, slot],
            wt_r.at[q, a + 1],
            (zflip(a) * 2 + y, tp),
        )

    def y_weight(q, k):
        own = isinstance(k, int) and k == 0
        here = chunk_dst(q, owner_of(k))
        return remote(
            chunk_src(q) if own else here,
            here,
            wy_s.at[q, k],
            wt_r.at[q, 1 if own else k + 3],
            ydev,
        )

    def sib_weight(q, k):
        own = isinstance(k, int) and k == 0
        here = chunk_dst(q, owner_of(k))
        return remote(chunk_src(q) if own else here, here, ws_s.at[q, k], wt_r.at[q, k], sib)

    def own_weight(q):
        return pltpu.make_async_copy(chunk_src(q), chunk_dst(q, sp), wt_r.at[q, 0])

    def wait_weight(q, k):
        ref = chunk_dst(q, owner_of(k))
        remote(ref, ref, wy_s.at[q, 0], wt_r.at[q, k], sib).wait_recv()

    inner = (z == 1) | (z == 2)
    near = 2
    middle = jnp.where(inner, 3, 4)
    far = jnp.where(inner, 4, 3)

    def forward_z(pairs):
        for q, k in pairs:
            with jax.named_scope(f"fz{q}_{2 if k is near else 3 if k is middle else 4}"):
                wait_weight(q, k)
            y_weight(q, k).start()
            sib_weight(q, k).start()

    def send_lead(q):
        z_weight(q, 0, 2).start()

    def send_other(first, last):
        for q in range(first, last):
            z_weight(q, 0, 1).start()
        for q in range(first, last):
            z_weight(q, 1, 3).start()

    @pl.when(lead)
    def _():
        for q in range(n_mix):
            send_lead(q)

    @pl.when(keep)
    def _():
        send_other(0, n_mix)

    gains[tp] = norm_gain[...]
    gain_peers = [(sp, lax.rem(tp + d, n_tp)) for d in range(1, n_tp)]

    def gain_copy(d):
        return remote(
            norm_gain, gains.at[tp], gain_s.at[d], gain_r.at[d], (sp, lax.rem(tp + d + 1, n_tp))
        )

    for d in range(n_tp - 1):
        gain_copy(d).start()

    def tap_copy():
        return remote(conv_taps, taps, tap_s.at[0], tap_r.at[0], sib)

    @pl.when(lead)
    def _():
        tap_copy().start()
        taps[...] = conv_taps[...]

    copies[2].wait()
    copies[3].wait()
    one = raw_qw[:, LANES : 2 * LANES].astype(jnp.float32)
    two = raw_qw[:, 2 * LANES :].astype(jnp.float32)
    turned_two = turn(two)
    qw[0, :, 0:LANES] = raw_qw[:, 0:LANES]
    qw[0, :, LANES:] = jnp.where(low, turn(one), 0.0).astype(jnp.bfloat16)
    qw[1, :, 0:LANES] = jnp.where(
        low, pltpu.roll(one, ROPE, 1), pltpu.roll(two, ROPE, 1)
    ).astype(jnp.bfloat16)
    qw[1, :, LANES:] = jnp.where(low, pltpu.roll(turned_two, ROPE, 1), 0.0).astype(jnp.bfloat16)
    for h in range(2):
        tile = raw_qn[:, h * LANES : (h + 1) * LANES].astype(jnp.float32)
        qn[h] = jnp.where(low, tile, turn(tile)).astype(jnp.bfloat16)
        vw[h, :, LANES:] = jnp.ones((rows, LANES), jnp.bfloat16)
    peak[...] = jnp.full(peak.shape, -1e30, jnp.float32)
    accw[...] = jnp.zeros(accw.shape, jnp.float32)
    accn[...] = jnp.zeros(accn.shape, jnp.float32)
    for i in (4, 5, 6, 7, 8):
        copies[i].wait()

    tile_rows = rows // 2

    def attend_tile(slot, query, key, value, acc, at, scale):
        scores = lax.dot_general(
            query, key, (((1,), (1,)), ((), ())), preferred_element_type=jnp.float32
        )
        before = peak[slot, at, :]
        after = jnp.maximum(before, jnp.max(scores, axis=-1, keepdims=True))
        pieces = [
            jnp.exp2((scores[:, j : j + LANES] - after) * scale)
            for j in range(0, scores.shape[1], LANES)
        ]
        spread = jnp.concatenate(pieces, axis=1).astype(jnp.bfloat16)
        keep = jnp.exp2((before - after) * scale)
        new = jnp.dot(spread, value, preferred_element_type=jnp.float32)
        for j in range(0, new.shape[1], LANES):
            acc[at, j : j + LANES] = acc[at, j : j + LANES] * keep + new[:, j : j + LANES]
        peak[slot, at, :] = after

    scale_w = (NOPE_W + ROPE) ** (-0.5) * math.log2(math.e)
    scale_n = (NOPE_N + ROPE) ** (-0.5) * math.log2(math.e)

    def block_step(i, carry):
        @pl.when(i == 1)
        @jax.named_scope("st0")
        def _():
            stage_one(i)
            stage_one(i + 1)
            stage_two(i)
            y_copy(i + 1).start()

        @pl.when((i == 3) & lead)
        def _():
            for q in range(n_all):
                y_weight(q, 0).start()
                sib_weight(q, 0).start()
                own_weight(q).start()

        for step, pairs in ((6, ((0, near),)),):

            @pl.when((i == step) & lead)
            def _():
                forward_z(pairs)

        @pl.when(i >= 1)
        @jax.named_scope("stA")
        def _():
            sib_copy(i).wait_recv()
            xs_copy(i).wait_recv()

        owner = owner_of(i)
        shared = lat_all[owner, :, 0:rank]
        rope = lat_all[owner, :, rank:].astype(jnp.float32)
        for h in range(2):
            pair = jnp.dot(
                shared,
                expand[:, h * 2 * LANES : (h + 1) * 2 * LANES],
                preferred_element_type=jnp.float32,
            )
            kw[h, :, 0:LANES] = pair[:, 0:LANES].astype(jnp.bfloat16)
            kw[h, :, LANES:] = lat_all[owner, :, rank:]
            vw[h, :, 0:LANES] = pair[:, LANES:].astype(jnp.bfloat16)
        pair = jnp.dot(shared, expand[:, wide_cols:], preferred_element_type=jnp.float32)
        for h in range(2):
            mine = pair[:, h * LANES : (h + 1) * LANES]
            kn[h] = jnp.where(low, mine, rope).astype(jnp.bfloat16)
            vn[h] = jnp.where(low, 1.0, mine).astype(jnp.bfloat16)

        def tile(t):
            at = pl.ds(t * tile_rows, tile_rows)
            for h in range(2):
                attend_tile(h, qw[h, at, :], kw[h], vw[h], accw.at[h], at, scale_w)
                attend_tile(2 + h, qn[h, at, :], kn[h], vn[h], accn.at[h], at, scale_n)

        tile(0)

        @pl.when((i >= 1) & (i <= 5))
        @jax.named_scope("st1")
        def _():
            stage_one(i + 2)

        @pl.when((i >= 1) & (i <= 2))
        def _():
            y_copy(i + 2).start()

        @pl.when((i >= 1) & (i <= 6))
        @jax.named_scope("st2")
        def _():
            stage_two(i + 1)

        tile(1)
        return carry

    lax.fori_loop(0, n_sp, block_step, 0)

    for h in range(2):
        heads[:, h * LANES : (h + 1) * LANES] = (
            accw[h, :, 0:LANES] / accw[h, :, LANES:]
        ).astype(jnp.bfloat16)
    first, second = accn[0], accn[1]
    first_r, second_r = pltpu.roll(first, ROPE, 1), pltpu.roll(second, ROPE, 1)
    heads[:, 2 * LANES :] = (
        jnp.where(low, first_r, second) / jnp.where(low, first, second_r)
    ).astype(jnp.bfloat16)

    step_rows = LANES
    n_steps = rows // step_rows

    def tile_at(t):
        return pl.ds(pl.multiple_of(t * step_rows, step_rows), step_rows)

    def part_copy(t):
        return remote(
            xsend.at[tile_at(t)], part_in.at[tile_at(t)], part_s.at[t], part_r.at[t], sib
        )

    def bx_copy(t):
        return remote(xsend.at[tile_at(t)], xrecv.at[tile_at(t)], bx_s.at[t], bx_r.at[t], xdev)

    pair_dev = (zflip(1) * 2 + y, tp)

    x_cols = n_tp // 2 * features

    def swap_copy(t):
        part = att.at[tile_at(t), pl.ds(pl.multiple_of(x * x_cols, x_cols), x_cols)]
        return remote(part, part, swap_s.at[t], swap_r.at[t], pair_dev)

    def cross_copy(t):
        part = att.at[tile_at(t), pl.ds(pl.multiple_of(x * x_cols, x_cols), x_cols)]
        return remote(part, part, cross_s.at[t], cross_r.at[t], xdev)

    @jax.named_scope("proj")
    def project(t, carry):
        at = tile_at(t)
        pieces = []
        for j in range(n_tp):
            cols = slice(j * features, (j + 1) * features)
            term = jnp.dot(heads[at, :], outcat[:, cols], preferred_element_type=jnp.float32)
            mine = jnp.where(tp == j, 1.0, 0.0)
            pieces.append(term + resid[at, :].astype(jnp.float32) * mine)

        @pl.when(lead)
        def _():
            for j in range(n_tp):
                cols = slice(j * features, (j + 1) * features)
                xsend[at, cols] = pieces[j].astype(jnp.bfloat16)
            part_copy(t).start()

        @pl.when(keep)
        def _():
            part_copy(t).wait_recv()
            for j in range(n_tp):
                cols = slice(j * features, (j + 1) * features)
                xsend[at, cols] = (
                    pieces[j] + part_in[at, cols].astype(jnp.float32)
                ).astype(jnp.bfloat16)
            bx_copy(t).start()

        return carry

    lax.fori_loop(0, n_steps, project, 0)

    def forward_y(q):
        with jax.named_scope(f"fy{q}"):
            for k in (1, 5, 6, 7):
                wait_weight(q, k)
                sib_weight(q, k).start()

    def halo_copy(side, plane):
        there = sp - 1 if side == 1 else sp + 1
        tz, ty = there // 2, there % 2
        src = att.at[pl.ds(0, HALO)] if side == 1 else att.at[pl.ds(rows - HALO, HALO)]
        dev = ((tz // 2 * 2 + plane) * 2 + ty, x * 2 + 1 - tz % 2)
        return remote(src, halo.at[side], halo_s.at[side, plane], halo_r.at[side], dev)

    def attq_copy(col):
        return remote(
            att.at[:, pl.ds(pl.multiple_of(col * features, features), features)],
            att_q,
            attq_s.at[0],
            attq_r.at[0],
            sib,
        )

    @jax.named_scope("exch")
    def exchange(t):
        at = tile_at(t)
        bx_copy(t).wait_recv()
        att[at, :] = (
            xsend[at, :].astype(jnp.float32) + xrecv[at, :].astype(jnp.float32)
        ).astype(jnp.bfloat16)
        swap_copy(t).start()

    def on_lead(*steps):
        @pl.when(lead)
        def _():
            for step, arg in steps:
                step(arg)

    def send_late(q):
        for q in range(n_mix, n_all):
            send_lead(q)

    @jax.named_scope("swapw")
    def swap_wait(tiles):
        for t in range(*tiles):
            swap_copy(t).wait_recv()
            cross_copy(t).start()

    @jax.named_scope("crossw")
    def cross_wait(q):
        for t in range(n_steps):
            cross_copy(t).wait_recv()

    on_lead(
        (forward_z, ((0, middle), (0, far), (1, near), (2, near), (3, near))),
        (forward_z, ((1, middle), (1, far))),
        (forward_z, ((2, middle), (2, far))),
        (forward_y, 0),
        (forward_z, ((3, middle), (3, far))),
        (send_late, 0),
        (swap_wait, (0, n_steps)),
        (forward_y, 1),
        (forward_y, 2),
        (cross_wait, 0),
    )

    @pl.when(keep)
    def _():
        for t in range(n_steps):
            exchange(t)

        @pl.when(sp > 0)
        def _():
            for plane in range(2):
                halo_copy(1, plane).start()

        @pl.when(sp < n_sp - 1)
        def _():
            for plane in range(2):
                halo_copy(0, plane).start()

        attq_copy(x * 2 + 1 - c).start()
        for q in range(n_mix, n_all):
            z_weight(q, 1, 3).start()
        for q in range(n_mix, n_all):
            z_weight(q, 0, 1).start()
        att_q[...] = att[:, pl.ds(pl.multiple_of(tp * features, features), features)]

    for d in range(n_tp - 1):
        gain_copy(d).wait_recv()

    def normalize(values):
        values = values.astype(jnp.float32)
        factor = lax.rsqrt(jnp.mean(values * values, axis=-1, keepdims=True) + epsilon)
        return jnp.concatenate(
            [
                values[:, j * features : (j + 1) * features] * factor * gains[j]
                for j in range(n_tp)
            ],
            axis=1,
        )

    def norm_step(t, carry):
        normed[tile_at(t), :] = normalize(att[tile_at(t), :]).astype(jnp.bfloat16)
        return carry

    lax.fori_loop(0, n_steps, norm_step, 0)

    def halo_wait(side):
        remote(
            halo.at[side], halo.at[side], halo_s.at[side, 0], halo_r.at[side], sib
        ).wait_recv()

    @pl.when(home > 0)
    @jax.named_scope("halo0")
    def _():
        halo_wait(0)

    @pl.when(home < n_sp - 1)
    @jax.named_scope("halo1")
    def _():
        halo_wait(1)

    previous = jnp.where(home > 0, normalize(halo[0])[HALO - 1 :, :], 0.0)
    following = jnp.where(home < n_sp - 1, normalize(halo[1])[0:1, :], 0.0)
    edge = lax.broadcasted_iota(jnp.int32, (HALO, width), 0)
    normed[rows:, :] = jnp.where(
        edge == 0, previous, jnp.where(edge == 1, following, 0.0)
    ).astype(jnp.bfloat16)

    def ready(part):
        for q in (2 * part, 2 * part + 1):
            own_weight(q).wait()

    def arrived(part):
        with jax.named_scope(f"arr{part}"):
            for q in (2 * part, 2 * part + 1):
                for k in range(n_sp):
                    wait_weight(q, k)

    on_lead((ready, 0))

    @pl.when(keep)
    def _():
        tap_copy().wait_recv()
        arrived(0)

    def smooth(values, cols, which):
        size = values.shape[1]
        row = lax.broadcasted_iota(jnp.int32, (rows, size), 0)
        values = values.astype(jnp.bfloat16).astype(jnp.float32)
        main = values[0:rows]
        before = jnp.where(row == 0, values[rows : rows + 1], pltpu.roll(main, 1, 0))
        after = jnp.where(
            row == rows - 1, values[rows + 1 : rows + 2], pltpu.roll(main, rows - 1, 0)
        )
        return (
            taps[0, which : which + 1, cols] * before
            + taps[1, which : which + 1, cols] * main
            + taps[2, which : which + 1, cols] * after
        )

    def mix(start, size):
        cols = pl.ds(start, size)
        both = []
        for m in range(2):
            rhs = wts[m, :, :, cols].reshape(width, size)
            both.append(
                smooth(jnp.dot(normed[...], rhs, preferred_element_type=jnp.float32), cols, m)
            )
        gate = both[0]
        hidden[:, cols] = (gate / (1.0 + jnp.exp(-gate)) * both[1]).astype(jnp.bfloat16)

    @jax.named_scope("mix")
    def mix_step(j, carry):
        mix(pl.multiple_of(j * block, block), block)
        return carry

    early = cut // block - 1
    lax.fori_loop(0, early, mix_step, 0)
    on_lead((forward_y, 3), (ready, 1))
    lax.fori_loop(early, cut // block, mix_step, 0)

    @pl.when(keep)
    def _():
        arrived(1)

    on_lead((forward_z, ((4, near), (4, middle), (4, far))))
    lax.fori_loop(cut // block, ff // block, mix_step, 0)
    if ff % block:
        mix(ff // block * block, ff % block)

    parts = features // depth
    source = jnp.where(home == sp, 0, 2) + x

    def out_slot(owner):
        half = owner % parts
        return source, slice(None), pl.ds(pl.multiple_of(half * depth, depth), depth)

    def out_copy(i, owner):
        return remote(
            osend.at[i],
            orecv.at[out_slot(owner)],
            out_s.at[i],
            out_r.at[source, owner % parts],
            (home, owner // parts),
        )

    def mine(owner):
        return (home == sp) & (owner // parts == tp)

    def order(step):
        far = (step >= 2) & (step != 5) & (step != 4) & (step != 7)
        near = (step == 4) | (step == 7)
        return jnp.where(far, step + 1, jnp.where(near, step - 2, jnp.where(step == 5, 6, step)))

    @jax.named_scope("down")
    def down_step(step, carry):
        i = order(step)

        @pl.when(lead & ((i == 1) | (i >= 5)))
        def _():
            for q in range(n_mix, n_all):
                wait_weight(q, i)
                sib_weight(q, i).start()

        @pl.when(lead & (i == 0))
        def _():
            for q in range(n_mix, n_all):
                own_weight(q).wait()

        @pl.when(keep)
        def _():
            for q in range(n_mix, n_all):
                wait_weight(q, i)

        owner = owner_of(i)
        term = lax.dot_general(
            hidden[...],
            wts[2, owner],
            (((1,), (1,)), ((), ())),
            preferred_element_type=jnp.float32,
        ).astype(jnp.bfloat16)

        @pl.when(mine(owner))
        def _():
            orecv[out_slot(owner)] = term

        @pl.when(jnp.logical_not(mine(owner)))
        def _():
            osend[i] = term
            out_copy(i, owner).start()

        return carry

    lax.fori_loop(0, 2, down_step, 0)
    on_lead((forward_z, ((5, near), (5, middle), (5, far))))
    lax.fori_loop(2, n_sp, down_step, 0)

    @pl.when(lead)
    def _():
        attq_copy(0).wait_recv()

    for s in range(orecv.shape[0]):

        @pl.when(lead | (s != source))
        @jax.named_scope("owait")
        def _():
            for half in range(parts):
                ref = orecv.at[s, :, pl.ds(half * depth, depth)]
                remote(ref, ref, out_s.at[0], out_r.at[s, half], sib).wait_recv()

    total = att_q[...].astype(jnp.float32)
    for s in range(orecv.shape[0]):
        total = total + orecv[s].astype(jnp.float32)
    result[...] = total.astype(jnp.bfloat16)
    store = pltpu.make_async_copy(result, output, local_sem.at[0])
    store.start()

    y_copy(0).wait_send()
    for i in (2, 3, 4):
        y_copy(i).wait_send()
    for a in (1, 2, 3):
        z_copy(a).wait_send()
    for i in range(1, n_sp):
        x_copy(i).wait_send()
        sib_copy(i).wait_send()
        xs_copy(i).wait_send()
    for d in range(n_tp - 1):
        gain_copy(d).wait_send()

    @pl.when(lead)
    def _():
        tap_copy().wait_send()
        for q in range(n_all):
            z_weight(q, 0, 2).wait_send()
            for k in (0, 2, 3, 4):
                y_weight(q, k).wait_send()
            for k in range(n_sp):
                sib_weight(q, k).wait_send()
        for t in range(n_steps):
            part_copy(t).wait_send()
            cross_copy(t).wait_send()

    @pl.when(keep)
    def _():
        attq_copy(0).wait_send()
        for q in range(n_all):
            z_weight(q, 0, 1).wait_send()
            z_weight(q, 1, 3).wait_send()
        for t in range(n_steps):
            bx_copy(t).wait_send()
            swap_copy(t).wait_send()

        @pl.when(sp > 0)
        def _():
            for plane in range(2):
                halo_copy(1, plane).wait_send()

        @pl.when(sp < n_sp - 1)
        def _():
            for plane in range(2):
                halo_copy(0, plane).wait_send()

    def out_wait(i, carry):
        owner = owner_of(i)

        @pl.when(jnp.logical_not(mine(owner)))
        def _():
            out_copy(i, owner).wait_send()

        return carry

    lax.fori_loop(0, n_sp, out_wait, 0)
    store.wait()


def fused_device(n_sp, n_tp, *arrays):
    (
        residual,
        query_wide,
        query_narrow,
        latent,
        rope_key,
        latent_gain,
        expand_wide,
        expand_narrow,
        out_wide,
        out_narrow,
        norm_gain,
        up_gate,
        up_value,
        down_weight,
        conv_taps,
    ) = arrays
    rows, features = residual.shape
    rank = latent.shape[1]
    depth, ff = up_gate.shape
    width = n_sp * depth
    fine, coarse = turn_tables(rows, n_sp)
    operands = (
        residual,
        query_wide,
        query_narrow,
        latent,
        rope_key,
        latent_gain[None],
        expand_wide,
        expand_narrow,
        out_wide,
        out_narrow,
        norm_gain[None],
        up_gate,
        up_value,
        down_weight,
        conv_taps,
        jnp.asarray(fine),
        jnp.asarray(coarse),
    )
    small = (5, 10, 14, 15, 16)
    anywhere = pl.BlockSpec(memory_space=pl.ANY)
    inside = pl.BlockSpec(memory_space=pltpu.VMEM)
    low, full = jnp.bfloat16, jnp.float32
    buffers = [
        ((n_sp, rows, rank + LANES), low),
        ((3, n_sp, depth, ff), low),
        ((rows, rank), low),
        ((rows, ROPE), low),
        (query_wide.shape, low),
        (query_narrow.shape, low),
        ((2, rows, 2 * LANES), low),
        ((2, rows, LANES), low),
        ((2, rows, 2 * LANES), low),
        ((2, rows, 2 * LANES), low),
        ((2, rows, LANES), low),
        ((2, rows, LANES), low),
        ((2, rows, 2 * LANES), full),
        ((2, rows, LANES), full),
        ((4, rows, LANES), full),
        ((rank, expand_wide.shape[1] + expand_narrow.shape[1]), low),
        ((out_wide.shape[0] + out_narrow.shape[0], width), low),
        ((rows, features), low),
        ((rows, out_wide.shape[0] + out_narrow.shape[0]), low),
        ((rows, width), low),
        ((rows, width), low),
        ((rows, width), low),
        ((rows, width), low),
        ((rows, features), low),
        ((rows + HALO, width), low),
        ((2, HALO, width), low),
        ((n_tp, 1, features), full),
        (conv_taps.shape, full),
        ((rows, ff), low),
        ((n_sp, rows, depth), low),
        ((4, rows, features), low),
        ((rows, features), low),
    ]
    steps = rows // LANES
    semaphores = [
        (9,),
        (8,),
        (8,),
        (8,),
        (8,),
        (3,),
        (5,),
        (8,),
        (8,),
        (8,),
        (6, 8),
        (6, 2),
        (6, 5),
        (6, 8),
        (steps,),
        (steps,),
        (steps,),
        (steps,),
        (steps,),
        (steps,),
        (steps,),
        (steps,),
        (2,),
        (2, 2),
        (1,),
        (1,),
        (3,),
        (3,),
        (1,),
        (1,),
        (4, features // depth),
        (8,),
    ]
    return pl.pallas_call(
        fused_kernel,
        out_shape=jax.ShapeDtypeStruct((rows, features), jnp.bfloat16),
        in_specs=[inside if i in small else anywhere for i in range(len(operands))],
        out_specs=anywhere,
        scratch_shapes=[pltpu.VMEM(shape, dtype) for shape, dtype in buffers]
        + [pltpu.SemaphoreType.DMA(shape) for shape in semaphores],
        compiler_params=pltpu.CompilerParams(
            collective_id=0, has_side_effects=True, vmem_limit_bytes=67043328
        ),
    )(*operands)


def solution(mesh):
    in_specs = (
        P("sp", "tp"),
        P("sp", "tp"),
        P("sp", "tp"),
        P("sp", None),
        P("sp", None),
        P(),
        P(None, "tp"),
        P(None, "tp"),
        P("tp", None),
        P("tp", None),
        P("tp"),
        P("sp", "tp"),
        P("sp", "tp"),
        P("sp", "tp"),
        P(None, None, "tp"),
    )
    out_specs = P("sp", "tp")
    n_sp, n_tp = mesh.shape["sp"], mesh.shape["tp"]
    body = per_device
    if (n_sp, n_tp) == (8, 4):
        body = functools.partial(fused_device, n_sp, n_tp)
    return jax.shard_map(
        body, mesh=mesh, in_specs=in_specs, out_specs=out_specs, check_vma=False
    )
```

```python
import functools
import math

import jax
import jax.numpy as jnp
import numpy as np
from jax import lax
from jax.experimental import pallas as pl
from jax.experimental.pallas import tpu as pltpu
from jax.sharding import PartitionSpec as P

D = 2048
ROPE = 64
NOPE_W = 128
VAL_W = 128
NOPE_N = 64
VAL_N = 64


theta = 10000.0
epsilon = 1e-06


def padded(block, sides, width):
    for axis, dim in sides:
        count = lax.axis_size(axis)
        forward = [(i, i + 1) for i in range(count - 1)]
        backward = [(target, source) for source, target in forward]
        low = lax.ppermute(
            lax.slice_in_dim(block, block.shape[dim] - width, None, axis=dim), axis, forward
        )
        high = lax.ppermute(lax.slice_in_dim(block, 0, width, axis=dim), axis, backward)
        block = jnp.concatenate([low, block, high], axis=dim)
    return block


def rotate(values, positions):
    half_dim = values.shape[-1] // 2
    inverse = jnp.power(
        jnp.float32(theta), -2.0 * jnp.arange(half_dim, dtype=jnp.float32) / values.shape[-1]
    )
    angles = positions[:, None] * inverse[None, :]
    new_shape = (angles.shape[0],) + (1,) * (values.ndim - 2) + (half_dim,)
    cosine = jnp.cos(angles).reshape(new_shape)
    sine_part = jnp.sin(angles).reshape(new_shape)
    floats = values.astype(jnp.float32)
    lower_half = floats[..., :half_dim]
    upper_half = floats[..., half_dim:]
    turned = jnp.concatenate(
        [
            lower_half * cosine - upper_half * sine_part,
            lower_half * sine_part + upper_half * cosine,
        ],
        axis=-1,
    )
    return turned.astype(jnp.bfloat16)


def turn_query(queries, head_count, nope_dim, positions):
    shaped = queries.reshape(queries.shape[0], head_count, nope_dim + ROPE)
    return jnp.concatenate(
        [shaped[..., :nope_dim], rotate(shaped[..., nope_dim:], positions)], axis=-1
    )


def attend_kernel(scale, chunk, q_ref, k_ref, v_ref, o_ref):
    query = q_ref[0]
    rows = query.shape[0]
    value_dim = v_ref.shape[-1]
    row_max = jnp.full((rows, 1), -1e30, jnp.float32)
    row_total = jnp.zeros((rows, 1), jnp.float32)
    weighted = jnp.zeros((rows, value_dim), jnp.float32)
    for start in range(0, k_ref.shape[1], chunk):
        scores = lax.dot_general(
            query,
            k_ref[0, start : start + chunk, :],
            (((1,), (1,)), ((), ())),
            preferred_element_type=jnp.float32,
        )
        new_max = jnp.maximum(row_max, jnp.max(scores, axis=-1, keepdims=True))
        weights = jnp.exp2((scores - new_max) * scale)
        keep = jnp.exp2((row_max - new_max) * scale)
        row_total = row_total * keep + jnp.sum(weights, axis=-1, keepdims=True)
        weighted = weighted * keep + jnp.dot(
            weights.astype(jnp.bfloat16),
            v_ref[0, start : start + chunk, :],
            preferred_element_type=jnp.float32,
        )
        row_max = new_max
    o_ref[0] = (weighted / row_total).astype(o_ref.dtype)


def attend(query, key, value, factor):
    heads, rows, width = query.shape
    count = key.shape[1]
    value_dim = value.shape[-1]
    block = math.gcd(rows, 320)
    chunk = math.gcd(count, 1024)
    return pl.pallas_call(
        functools.partial(attend_kernel, factor * math.log2(math.e), chunk),
        grid=(heads, rows // block),
        in_specs=[
            pl.BlockSpec((1, block, width), lambda h, i: (h, i, 0)),
            pl.BlockSpec((1, count, width), lambda h, i: (h, 0, 0)),
            pl.BlockSpec((1, count, value_dim), lambda h, i: (h, 0, 0)),
        ],
        out_specs=pl.BlockSpec((1, block, value_dim), lambda h, i: (h, i, 0)),
        out_shape=jax.ShapeDtypeStruct((heads, rows, value_dim), jnp.bfloat16),
        compiler_params=pltpu.CompilerParams(
            dimension_semantics=("arbitrary", "arbitrary"), vmem_limit_bytes=48 << 20
        ),
        cost_estimate=pl.CostEstimate(
            flops=2 * heads * rows * count * 512,
            bytes_accessed=2 * heads * count * (width + value_dim),
            transcendentals=heads * rows * count,
        ),
    )(query, key, value)


def key_value(latent, expand, head_count, key_dim, rope):
    pair = expand.reshape(expand.shape[0], head_count, -1)
    key = jnp.einsum(
        "td,dhn->htn", latent, pair[..., :key_dim], preferred_element_type=jnp.float32
    ).astype(jnp.bfloat16)
    value = jnp.einsum(
        "td,dhn->htn", latent, pair[..., key_dim:], preferred_element_type=jnp.float32
    ).astype(jnp.bfloat16)
    shared = jnp.broadcast_to(rope[None], (head_count,) + rope.shape)
    return jnp.concatenate([key, shared], axis=-1), value


def side_by_side(heads):
    return jnp.transpose(heads, (1, 0, 2)).reshape(heads.shape[1], -1)


def per_device(
    residual,
    query_wide,
    query_narrow,
    latent,
    rope_key,
    latent_gain,
    expand_wide,
    expand_narrow,
    out_wide,
    out_narrow,
    norm_gain,
    up_gate,
    up_value,
    down_weight,
    conv_taps,
):
    tok_rows = residual.shape[0]
    offset = lax.axis_index("sp") * tok_rows
    positions = (offset + lax.iota(jnp.int32, tok_rows)).astype(jnp.float32)
    latent_float = latent.astype(jnp.float32)
    normed_latent = (
        latent_float
        * lax.rsqrt(jnp.mean(latent_float * latent_float, axis=-1, keepdims=True) + epsilon)
        * latent_gain
    ).astype(jnp.bfloat16)
    rope_turned = rotate(rope_key, positions)
    wide_heads = query_wide.shape[1] // (NOPE_W + ROPE)
    narrow_heads = query_narrow.shape[1] // (NOPE_N + ROPE)
    query_w = turn_query(query_wide, wide_heads, NOPE_W, positions)
    query_n = turn_query(query_narrow, narrow_heads, NOPE_N, positions)
    gathered = lax.all_gather(
        jnp.concatenate([normed_latent, rope_turned, jnp.zeros_like(rope_turned)], axis=1),
        "sp",
        axis=0,
        tiled=True,
    )
    full_gain = lax.all_gather(norm_gain, "tp", axis=0, tiled=True)
    gathered, up_gate, up_value, down_weight = lax.optimization_barrier(
        (gathered, up_gate, up_value, down_weight)
    )
    gate_full, value_full, down_full = (
        lax.all_gather(up_gate, "sp", axis=0, tiled=True),
        lax.all_gather(up_value, "sp", axis=0, tiled=True),
        lax.all_gather(down_weight, "sp", axis=0, tiled=True),
    )
    rank = latent.shape[1]
    latent_all, rope_all = gathered[:, :rank], gathered[:, rank : rank + ROPE]
    key_w, value_w = key_value(latent_all, expand_wide, wide_heads, NOPE_W, rope_all)
    key_n, value_n = key_value(latent_all, expand_narrow, narrow_heads, NOPE_N, rope_all)
    heads_wide = side_by_side(
        attend(jnp.transpose(query_w, (1, 0, 2)), key_w, value_w, (NOPE_W + ROPE) ** (-0.5))
    )
    heads_narrow = side_by_side(
        attend(jnp.transpose(query_n, (1, 0, 2)), key_n, value_n, (NOPE_N + ROPE) ** (-0.5))
    )
    head_terms = jnp.dot(heads_wide, out_wide, preferred_element_type=jnp.float32)
    head_terms = head_terms + jnp.dot(heads_narrow, out_narrow, preferred_element_type=jnp.float32)
    head_terms, gate_full, value_full = lax.optimization_barrier(
        (head_terms.astype(jnp.bfloat16), gate_full, value_full)
    )
    head_shares = lax.psum_scatter(
        head_terms, "tp", scatter_dimension=1, tiled=True
    ).astype(jnp.float32)
    attended = (residual.astype(jnp.float32) + head_shares).astype(jnp.bfloat16)
    attended_float = attended.astype(jnp.float32)
    attended_full = lax.all_gather(attended, "tp", axis=1, tiled=True).astype(jnp.float32)
    squares = jnp.mean(attended_full * attended_full, axis=-1, keepdims=True)
    normed_full = (attended_full * lax.rsqrt(squares + epsilon) * full_gain).astype(jnp.bfloat16)
    gate_float = jnp.dot(normed_full, gate_full, preferred_element_type=jnp.float32)
    value_float = jnp.dot(normed_full, value_full, preferred_element_type=jnp.float32)
    gate_width = up_gate.shape[1]
    both_up = jnp.concatenate(
        [gate_float.astype(jnp.bfloat16), value_float.astype(jnp.bfloat16)], axis=1
    )
    extended = padded(both_up, (("sp", 0),), 1).astype(jnp.float32)
    tap_rows = conv_taps.reshape(3, 2 * gate_width)
    smoothed = (
        tap_rows[0] * extended[:-2] + tap_rows[1] * extended[1:-1] + tap_rows[2] * extended[2:]
    )
    hidden = (jax.nn.silu(smoothed[:, :gate_width]) * smoothed[:, gate_width:]).astype(jnp.bfloat16)
    unit_terms = lax.dot_general(
        hidden, down_full, (((1,), (1,)), ((), ())), preferred_element_type=jnp.float32
    )
    unit_shares = lax.psum_scatter(
        unit_terms.astype(jnp.bfloat16), "tp", scatter_dimension=1, tiled=True
    ).astype(jnp.float32)
    return (attended_float + unit_shares).astype(jnp.bfloat16)


MESH = pl.DeviceIdType.MESH
LANES = 128
HALO = 16


def turn_tables(rows, groups):
    half = ROPE // 2
    inverse = np.power(theta, -2.0 * np.arange(half) / ROPE)
    inverse = np.tile(inverse, LANES // half)[None, :]
    local = np.arange(rows)[:, None] * inverse
    start = (np.arange(groups) * rows)[:, None] * inverse
    fine = np.stack([np.cos(local), np.sin(local)]).astype(np.float32)
    coarse = np.stack([np.cos(start), np.sin(start)]).astype(np.float32)
    return fine, coarse


def swap_halves(values, lane):
    half = ROPE // 2
    left = pltpu.roll(values, LANES - half, 1)
    right = pltpu.roll(values, half, 1)
    return jnp.where(lane % ROPE < half, left, right)


def fused_kernel(
    residual,
    query_wide,
    query_narrow,
    latent,
    rope_key,
    latent_gain,
    expand_wide,
    expand_narrow,
    out_wide,
    out_narrow,
    norm_gain,
    up_gate,
    up_value,
    down_weight,
    conv_taps,
    fine_tab,
    coarse_tab,
    output,
    lat_all,
    wts,
    raw_lat,
    raw_rope,
    raw_qw,
    raw_qn,
    qw,
    qn,
    kw,
    vw,
    kn,
    vn,
    accw,
    accn,
    peak,
    expand,
    outcat,
    resid,
    heads,
    part_in,
    xsend,
    xrecv,
    att,
    att_q,
    normed,
    halo,
    gains,
    taps,
    hidden,
    osend,
    orecv,
    result,
    local_sem,
    own_r,
    sib_r,
    x_r,
    xs_r,
    z_s,
    zf_s,
    y_s,
    sib_s,
    x_s,
    xs_s,
    wt_r,
    wz_s,
    wy_s,
    ws_s,
    part_r,
    part_s,
    bx_r,
    bx_s,
    swap_r,
    swap_s,
    cross_r,
    cross_s,
    halo_r,
    halo_s,
    attq_r,
    attq_s,
    gain_r,
    gain_s,
    tap_r,
    tap_s,
    out_r,
    out_s,
):
    sp = lax.axis_index("sp")
    tp = lax.axis_index("tp")
    n_sp = wts.shape[1]
    n_tp = gains.shape[0]
    z, y, x, c = sp // 2, sp % 2, tp // 2, tp % 2
    leader = z % 2
    lead = c == leader
    keep = c != leader
    home = (z // 2 * 2 + 1 - c) * 2 + y
    rows, rank = raw_lat.shape
    quarter = rows // n_tp
    weights = (up_gate, up_value, down_weight)
    depth, ff = up_gate.shape
    width = n_sp * depth
    features = resid.shape[1]
    sib = (sp, x * 2 + 1 - c)
    xdev = (sp, (1 - x) * 2 + c)
    ydev = (z * 2 + 1 - y, tp)

    def zflip(a):
        return jnp.where(a == 1, z // 2 * 2 + 1 - z % 2, jnp.where(a == 2, (z + 2) % 4, 3 - z))

    def remote(src, dst, ss, rs, dev):
        return pltpu.make_async_remote_copy(
            src_ref=src, dst_ref=dst, send_sem=ss, recv_sem=rs, device_id=dev, device_id_type=MESH
        )

    barrier = pltpu.get_barrier_semaphore()
    for ds_ in range(n_sp):
        for dt in range(n_tp):
            if ds_ or dt:
                pl.semaphore_signal(
                    barrier,
                    inc=1,
                    device_id=(lax.rem(sp + ds_, n_sp), lax.rem(tp + dt, n_tp)),
                    device_id_type=MESH,
                )

    wide_cols = expand_wide.shape[1]
    loads = [
        (latent, raw_lat),
        (rope_key, raw_rope),
        (query_wide, raw_qw),
        (query_narrow, raw_qn),
        (expand_wide, expand.at[:, pl.ds(0, wide_cols)]),
        (expand_narrow, expand.at[:, pl.ds(wide_cols, expand_narrow.shape[1])]),
        (out_wide, outcat.at[pl.ds(0, out_wide.shape[0])]),
        (out_narrow, outcat.at[pl.ds(out_wide.shape[0], out_narrow.shape[0])]),
        (residual, resid),
    ]
    copies = [
        pltpu.make_async_copy(src, dst, local_sem.at[i]) for i, (src, dst) in enumerate(loads)
    ]
    for copy in copies:
        copy.start()

    lane = lax.broadcasted_iota(jnp.int32, (rows, LANES), 1)
    low = lane < ROPE
    copies[0].wait()
    copies[1].wait()
    base = coarse_tab[:, pl.ds(sp, 1), :]
    cosine = base[0] * fine_tab[0] - base[1] * fine_tab[1]
    sine = base[1] * fine_tab[0] + base[0] * fine_tab[1]
    sine = jnp.where(lane % ROPE < ROPE // 2, -sine, sine)

    def turn(values):
        return values * cosine + swap_halves(values, lane) * sine

    lat_f = raw_lat[...].astype(jnp.float32)
    square = jnp.mean(lat_f * lat_f, axis=-1, keepdims=True)
    lat_all[sp, :, 0:rank] = (lat_f * lax.rsqrt(square + epsilon) * latent_gain[...]).astype(
        jnp.bfloat16
    )
    rope_f = raw_rope[...].astype(jnp.float32).T
    rope_f = jnp.concatenate([rope_f, rope_f], axis=1)
    lat_all[sp, :, rank:] = turn(rope_f).astype(jnp.bfloat16)

    with jax.named_scope("barw"):
        pl.semaphore_wait(barrier, n_sp * n_tp - 1)

    def piece(owner, who):
        return lat_all.at[owner, pl.ds(pl.multiple_of(who * quarter, quarter), quarter)]

    inner = (z == 1) | (z == 2)

    def z_copy(a):
        own = piece(sp, tp)
        return remote(own, own, z_s.at[a], own_r.at[2 if a == 1 else 3], (zflip(a) * 2 + y, tp))

    def z_onward(i):
        block = piece(lat_owner(i), tp)
        to = jnp.where(i == 2, zflip(3), zflip(1))
        return remote(
            block, block, zf_s.at[i], own_r.at[jnp.where(i == 2, 4, i)], (to * 2 + y, tp)
        )

    def lat_owner(i):
        b = jnp.where((i == 1) | (i >= 5), 1, 0)
        p = jnp.where(i <= 1, 0, jnp.where(i <= 4, i, i - 3))
        late = jnp.where((p == 3) == inner, 3, 2)
        oz = jnp.where(p == 0, z, jnp.where(p == 2, zflip(1), zflip(late)))
        return oz * 2 + jnp.where(b == 1, 1 - y, y)

    def owner_of(i):
        b = jnp.where((i == 1) | (i >= 5), 1, 0)
        a = jnp.where(i <= 1, 0, jnp.where(i <= 4, i - 1, i - 4))
        oz = jnp.where(a == 0, z, zflip(a))
        return oz * 2 + jnp.where(b == 1, 1 - y, y)

    def y_copy(i):
        own = piece(lat_owner(i), tp)
        return remote(own, own, y_s.at[i], own_r.at[jnp.where(i == 0, 1, i + 3)], ydev)

    def sib_copy(i):
        own = piece(lat_owner(i), tp)
        return remote(own, own, sib_s.at[i], sib_r.at[i], sib)

    def x_copy(i):
        own = piece(lat_owner(i), tp)
        return remote(own, own, x_s.at[i], x_r.at[i], xdev)

    def xs_copy(i):
        other = piece(lat_owner(i), (1 - x) * 2 + c)
        return remote(other, other, xs_s.at[i], xs_r.at[i], sib)

    def stage_one(i):
        arrival = piece(lat_owner(i), tp)
        remote(arrival, arrival, y_s.at[0], own_r.at[i], sib).wait_recv()

        @pl.when((i >= 2) & (i <= 4) & inner)
        def _():
            z_onward(i).start()

        @pl.when((i >= 2) & (i <= 4))
        def _():
            y_copy(i).start()

        x_copy(i).start()
        sib_copy(i).start()

    def stage_two(i):
        x_copy(i).wait_recv()
        xs_copy(i).start()

    y_copy(0).start()
    z_copy(1).start()

    @pl.when(inner)
    def _():
        z_copy(3).start()

    block = 2 * LANES
    cut = (ff // block + 1) // 2 * block
    half_depth = depth // 2
    col_parts = (pl.ds(0, cut), pl.ds(cut, ff - cut))
    row_parts = (pl.ds(0, half_depth), pl.ds(half_depth, half_depth))
    n_mix, n_all = 4, 6

    def chunk_src(q):
        if q < n_mix:
            return weights[q % 2].at[:, col_parts[q // 2]]
        return weights[2].at[row_parts[q - n_mix]]

    def chunk_dst(q, owner):
        if q < n_mix:
            return wts.at[q % 2, owner, :, col_parts[q // 2]]
        return wts.at[2, owner, row_parts[q - n_mix]]

    def z_weight(q, slot, a):
        return remote(
            chunk_src(q),
            chunk_dst(q, sp),
            wz_s.at[q, slot],
            wt_r.at[q, a + 1],
            (zflip(a) * 2 + y, tp),
        )

    def y_weight(q, k):
        own = isinstance(k, int) and k == 0
        here = chunk_dst(q, owner_of(k))
        return remote(
            chunk_src(q) if own else here,
            here,
            wy_s.at[q, k],
            wt_r.at[q, 1 if own else k + 3],
            ydev,
        )

    def sib_weight(q, k):
        own = isinstance(k, int) and k == 0
        here = chunk_dst(q, owner_of(k))
        return remote(chunk_src(q) if own else here, here, ws_s.at[q, k], wt_r.at[q, k], sib)

    def own_weight(q):
        return pltpu.make_async_copy(chunk_src(q), chunk_dst(q, sp), wt_r.at[q, 0])

    def wait_weight(q, k):
        ref = chunk_dst(q, owner_of(k))
        remote(ref, ref, wy_s.at[q, 0], wt_r.at[q, k], sib).wait_recv()

    near = 2
    middle = jnp.where(inner, 3, 4)
    far = jnp.where(inner, 4, 3)

    def forward_z(pairs):
        for q, k in pairs:
            with jax.named_scope(f"fz{q}_{2 if k is near else 3 if k is middle else 4}"):
                wait_weight(q, k)
            y_weight(q, k).start()
            sib_weight(q, k).start()

    def send_lead(q):
        z_weight(q, 0, 2).start()

    def send_other(first, last):
        for q in range(first, last):
            z_weight(q, 0, 1).start()
        for q in range(first, last):
            z_weight(q, 1, 3).start()


    outer = jnp.logical_not(inner)

    @pl.when(outer & lead)
    def _():
        for q in range(n_mix):
            send_lead(q)

    @pl.when(outer & keep)
    def _():
        send_other(0, n_mix)

    gains[tp] = norm_gain[...]
    gain_peers = [(sp, lax.rem(tp + d, n_tp)) for d in range(1, n_tp)]

    def gain_copy(d):
        return remote(
            norm_gain, gains.at[tp], gain_s.at[d], gain_r.at[d], (sp, lax.rem(tp + d + 1, n_tp))
        )

    for d in range(n_tp - 1):
        gain_copy(d).start()

    def tap_copy():
        return remote(conv_taps, taps, tap_s.at[0], tap_r.at[0], sib)

    @pl.when(lead)
    def _():
        tap_copy().start()
        taps[...] = conv_taps[...]

    copies[2].wait()
    copies[3].wait()
    one = raw_qw[:, LANES : 2 * LANES].astype(jnp.float32)
    two = raw_qw[:, 2 * LANES :].astype(jnp.float32)
    turned_two = turn(two)
    qw[0, :, 0:LANES] = raw_qw[:, 0:LANES]
    qw[0, :, LANES:] = jnp.where(low, turn(one), 0.0).astype(jnp.bfloat16)
    qw[1, :, 0:LANES] = jnp.where(
        low, pltpu.roll(one, ROPE, 1), pltpu.roll(two, ROPE, 1)
    ).astype(jnp.bfloat16)
    qw[1, :, LANES:] = jnp.where(low, pltpu.roll(turned_two, ROPE, 1), 0.0).astype(jnp.bfloat16)
    for h in range(2):
        tile = raw_qn[:, h * LANES : (h + 1) * LANES].astype(jnp.float32)
        qn[h] = jnp.where(low, tile, turn(tile)).astype(jnp.bfloat16)
        vw[h, :, LANES:] = jnp.ones((rows, LANES), jnp.bfloat16)
    peak[...] = jnp.full(peak.shape, -1e30, jnp.float32)
    accw[...] = jnp.zeros(accw.shape, jnp.float32)
    accn[...] = jnp.zeros(accn.shape, jnp.float32)
    for i in (4, 5, 6, 7, 8):
        copies[i].wait()

    tile_rows = rows // 2

    def attend_tile(slot, query, key, value, acc, at, scale):
        scores = lax.dot_general(
            query, key, (((1,), (1,)), ((), ())), preferred_element_type=jnp.float32
        )
        before = peak[slot, at, :]
        after = jnp.maximum(before, jnp.max(scores, axis=-1, keepdims=True))
        pieces = [
            jnp.exp2((scores[:, j : j + LANES] - after) * scale)
            for j in range(0, scores.shape[1], LANES)
        ]
        spread = jnp.concatenate(pieces, axis=1).astype(jnp.bfloat16)
        keep = jnp.exp2((before - after) * scale)
        new = jnp.dot(spread, value, preferred_element_type=jnp.float32)
        for j in range(0, new.shape[1], LANES):
            acc[at, j : j + LANES] = acc[at, j : j + LANES] * keep + new[:, j : j + LANES]
        peak[slot, at, :] = after

    scale_w = (NOPE_W + ROPE) ** (-0.5) * math.log2(math.e)
    scale_n = (NOPE_N + ROPE) ** (-0.5) * math.log2(math.e)

    def block_step(i, carry):
        @pl.when(i == 1)
        @jax.named_scope("st0")
        def _():
            stage_one(i)
            stage_one(i + 1)

            @pl.when(inner)
            def _():
                stage_one(i + 2)

            stage_two(i)

        @pl.when((i == 3) & lead)
        def _():
            for q in range(n_all):
                y_weight(q, 0).start()
                sib_weight(q, 0).start()
                own_weight(q).start()

        for step, pairs in ((6, ((0, near),)),):

            @pl.when((i == step) & lead)
            def _():
                forward_z(pairs)

        @pl.when(i >= 1)
        @jax.named_scope("stA")
        def _():
            sib_copy(i).wait_recv()
            xs_copy(i).wait_recv()

        owner = lat_owner(i)
        shared = lat_all[owner, :, 0:rank]
        rope = lat_all[owner, :, rank:].astype(jnp.float32)
        for h in range(2):
            pair = jnp.dot(
                shared,
                expand[:, h * 2 * LANES : (h + 1) * 2 * LANES],
                preferred_element_type=jnp.float32,
            )
            kw[h, :, 0:LANES] = pair[:, 0:LANES].astype(jnp.bfloat16)
            kw[h, :, LANES:] = lat_all[owner, :, rank:]
            vw[h, :, 0:LANES] = pair[:, LANES:].astype(jnp.bfloat16)
        pair = jnp.dot(shared, expand[:, wide_cols:], preferred_element_type=jnp.float32)
        for h in range(2):
            mine = pair[:, h * LANES : (h + 1) * LANES]
            kn[h] = jnp.where(low, mine, rope).astype(jnp.bfloat16)
            vn[h] = jnp.where(low, 1.0, mine).astype(jnp.bfloat16)

        def tile(t):
            at = pl.ds(t * tile_rows, tile_rows)
            for h in range(2):
                attend_tile(h, qw[h, at, :], kw[h], vw[h], accw.at[h], at, scale_w)
                attend_tile(2 + h, qn[h, at, :], kn[h], vn[h], accn.at[h], at, scale_n)

        tile(0)

        ahead = i + jnp.where(inner, 3, 2)

        @pl.when((i >= 1) & (ahead < n_sp))
        @jax.named_scope("st1")
        def _():
            stage_one(ahead)

        @pl.when((i == 1) & inner & lead)
        def _():
            for q in range(n_mix):
                send_lead(q)

        @pl.when((i == 1) & inner & keep)
        def _():
            send_other(0, n_mix)

        @pl.when((i >= 1) & (i <= 6))
        @jax.named_scope("st2")
        def _():
            stage_two(i + 1)

        tile(1)
        return carry

    lax.fori_loop(0, n_sp, block_step, 0)

    for h in range(2):
        heads[:, h * LANES : (h + 1) * LANES] = (
            accw[h, :, 0:LANES] / accw[h, :, LANES:]
        ).astype(jnp.bfloat16)
    first, second = accn[0], accn[1]
    first_r, second_r = pltpu.roll(first, ROPE, 1), pltpu.roll(second, ROPE, 1)
    heads[:, 2 * LANES :] = (
        jnp.where(low, first_r, second) / jnp.where(low, first, second_r)
    ).astype(jnp.bfloat16)

    step_rows = LANES
    n_steps = rows // step_rows

    def tile_at(t):
        return pl.ds(pl.multiple_of(t * step_rows, step_rows), step_rows)

    def part_copy(t):
        return remote(
            xsend.at[tile_at(t)], part_in.at[tile_at(t)], part_s.at[t], part_r.at[t], sib
        )

    def bx_copy(t):
        return remote(xsend.at[tile_at(t)], xrecv.at[tile_at(t)], bx_s.at[t], bx_r.at[t], xdev)

    pair_dev = (zflip(1) * 2 + y, tp)

    x_cols = n_tp // 2 * features

    def swap_copy(t):
        part = att.at[tile_at(t), pl.ds(pl.multiple_of(x * x_cols, x_cols), x_cols)]
        return remote(part, part, swap_s.at[t], swap_r.at[t], pair_dev)

    def cross_copy(t):
        part = att.at[tile_at(t), pl.ds(pl.multiple_of(x * x_cols, x_cols), x_cols)]
        return remote(part, part, cross_s.at[t], cross_r.at[t], xdev)

    @jax.named_scope("proj")
    def project(t, carry):
        at = tile_at(t)
        pieces = []
        for j in range(n_tp):
            cols = slice(j * features, (j + 1) * features)
            term = jnp.dot(heads[at, :], outcat[:, cols], preferred_element_type=jnp.float32)
            mine = jnp.where(tp == j, 1.0, 0.0)
            pieces.append(term + resid[at, :].astype(jnp.float32) * mine)

        @pl.when(lead)
        def _():
            for j in range(n_tp):
                cols = slice(j * features, (j + 1) * features)
                xsend[at, cols] = pieces[j].astype(jnp.bfloat16)
            part_copy(t).start()

        @pl.when(keep)
        def _():
            part_copy(t).wait_recv()
            for j in range(n_tp):
                cols = slice(j * features, (j + 1) * features)
                xsend[at, cols] = (
                    pieces[j] + part_in[at, cols].astype(jnp.float32)
                ).astype(jnp.bfloat16)
            bx_copy(t).start()

        return carry

    lax.fori_loop(0, n_steps, project, 0)

    def forward_y(q):
        with jax.named_scope(f"fy{q}"):
            for k in (1, 5, 6, 7):
                wait_weight(q, k)
                sib_weight(q, k).start()

    def halo_copy(side, plane):
        there = sp - 1 if side == 1 else sp + 1
        tz, ty = there // 2, there % 2
        src = att.at[pl.ds(0, HALO)] if side == 1 else att.at[pl.ds(rows - HALO, HALO)]
        dev = ((tz // 2 * 2 + plane) * 2 + ty, x * 2 + 1 - tz % 2)
        return remote(src, halo.at[side], halo_s.at[side, plane], halo_r.at[side], dev)

    def attq_copy(col):
        return remote(
            att.at[:, pl.ds(pl.multiple_of(col * features, features), features)],
            att_q,
            attq_s.at[0],
            attq_r.at[0],
            sib,
        )

    @jax.named_scope("exch")
    def exchange(t):
        at = tile_at(t)
        bx_copy(t).wait_recv()
        att[at, :] = (
            xsend[at, :].astype(jnp.float32) + xrecv[at, :].astype(jnp.float32)
        ).astype(jnp.bfloat16)
        swap_copy(t).start()

    def on_lead(*steps):
        @pl.when(lead)
        def _():
            for step, arg in steps:
                step(arg)

    def send_late(q):
        for q in range(n_mix, n_all):
            send_lead(q)

    @jax.named_scope("swapw")
    def swap_wait(tiles):
        for t in range(*tiles):
            swap_copy(t).wait_recv()
            cross_copy(t).start()

    @jax.named_scope("crossw")
    def cross_wait(q):
        for t in range(n_steps):
            cross_copy(t).wait_recv()

    on_lead(
        (forward_z, ((0, middle), (0, far), (1, near), (2, near), (3, near))),
        (forward_z, ((1, middle), (1, far))),
        (forward_z, ((2, middle), (2, far))),
        (forward_y, 0),
        (forward_z, ((3, middle), (3, far))),
        (send_late, 0),
        (forward_y, 1),
        (swap_wait, (0, n_steps)),
        (forward_y, 2),
        (forward_y, 3),
        (cross_wait, 0),
    )

    @pl.when(keep)
    def _():
        for t in range(n_steps):
            exchange(t)

        @pl.when(sp > 0)
        def _():
            for plane in range(2):
                halo_copy(1, plane).start()

        @pl.when(sp < n_sp - 1)
        def _():
            for plane in range(2):
                halo_copy(0, plane).start()

        attq_copy(x * 2 + 1 - c).start()
        for q in range(n_mix, n_all):
            z_weight(q, 1, 3).start()
        for q in range(n_mix, n_all):
            z_weight(q, 0, 1).start()
        att_q[...] = att[:, pl.ds(pl.multiple_of(tp * features, features), features)]

    for d in range(n_tp - 1):
        gain_copy(d).wait_recv()

    def normalize(values):
        values = values.astype(jnp.float32)
        factor = lax.rsqrt(jnp.mean(values * values, axis=-1, keepdims=True) + epsilon)
        return jnp.concatenate(
            [
                values[:, j * features : (j + 1) * features] * factor * gains[j]
                for j in range(n_tp)
            ],
            axis=1,
        )

    def norm_step(t, carry):
        normed[tile_at(t), :] = normalize(att[tile_at(t), :]).astype(jnp.bfloat16)
        return carry

    lax.fori_loop(0, n_steps, norm_step, 0)

    def halo_wait(side):
        remote(
            halo.at[side], halo.at[side], halo_s.at[side, 0], halo_r.at[side], sib
        ).wait_recv()

    @pl.when(home > 0)
    @jax.named_scope("halo0")
    def _():
        halo_wait(0)

    @pl.when(home < n_sp - 1)
    @jax.named_scope("halo1")
    def _():
        halo_wait(1)

    previous = jnp.where(home > 0, normalize(halo[0])[HALO - 1 :, :], 0.0)
    following = jnp.where(home < n_sp - 1, normalize(halo[1])[0:1, :], 0.0)
    edge = lax.broadcasted_iota(jnp.int32, (HALO, width), 0)
    normed[rows:, :] = jnp.where(
        edge == 0, previous, jnp.where(edge == 1, following, 0.0)
    ).astype(jnp.bfloat16)

    def ready(part):
        for q in (2 * part, 2 * part + 1):
            own_weight(q).wait()

    def arrived(part):
        with jax.named_scope(f"arr{part}"):
            for q in (2 * part, 2 * part + 1):
                for k in range(n_sp):
                    wait_weight(q, k)

    on_lead((ready, 0))

    @pl.when(keep)
    def _():
        tap_copy().wait_recv()
        arrived(0)

    def smooth(values, cols, which):
        size = values.shape[1]
        row = lax.broadcasted_iota(jnp.int32, (rows, size), 0)
        values = values.astype(jnp.bfloat16).astype(jnp.float32)
        main = values[0:rows]
        before = jnp.where(row == 0, values[rows : rows + 1], pltpu.roll(main, 1, 0))
        after = jnp.where(
            row == rows - 1, values[rows + 1 : rows + 2], pltpu.roll(main, rows - 1, 0)
        )
        return (
            taps[0, which : which + 1, cols] * before
            + taps[1, which : which + 1, cols] * main
            + taps[2, which : which + 1, cols] * after
        )

    def mix(start, size):
        cols = pl.ds(start, size)
        both = []
        for m in range(2):
            rhs = wts[m, :, :, cols].reshape(width, size)
            both.append(
                smooth(jnp.dot(normed[...], rhs, preferred_element_type=jnp.float32), cols, m)
            )
        gate = both[0]
        hidden[:, cols] = (gate / (1.0 + jnp.exp(-gate)) * both[1]).astype(jnp.bfloat16)

    @jax.named_scope("mix")
    def mix_step(j, carry):
        mix(pl.multiple_of(j * block, block), block)
        return carry

    early = cut // block - 1
    lax.fori_loop(0, early, mix_step, 0)
    on_lead((ready, 1), (forward_z, ((4, near), (4, middle))))
    lax.fori_loop(early, cut // block, mix_step, 0)

    @pl.when(keep)
    def _():
        arrived(1)

    on_lead((forward_z, ((4, far),)))
    lax.fori_loop(cut // block, ff // block, mix_step, 0)
    if ff % block:
        mix(ff // block * block, ff % block)

    on_lead((forward_z, ((5, near), (5, middle))))

    parts = features // depth
    source = jnp.where(home == sp, 0, 2) + x

    def out_slot(owner):
        half = owner % parts
        return source, slice(None), pl.ds(pl.multiple_of(half * depth, depth), depth)

    def out_copy(i, owner):
        return remote(
            osend.at[i],
            orecv.at[out_slot(owner)],
            out_s.at[i],
            out_r.at[source, owner % parts],
            (home, owner // parts),
        )

    def mine(owner):
        return (home == sp) & (owner // parts == tp)

    def order(step):
        far = (step >= 2) & (step != 5) & (step != 4) & (step != 7)
        near = (step == 4) | (step == 7)
        return jnp.where(far, step + 1, jnp.where(near, step - 2, jnp.where(step == 5, 6, step)))

    @jax.named_scope("down")
    def down_step(step, carry):
        i = order(step)

        @pl.when(lead & ((i == 1) | (i >= 5)))
        def _():
            for q in range(n_mix, n_all):
                wait_weight(q, i)
                sib_weight(q, i).start()

        @pl.when(lead & (i == 0))
        def _():
            for q in range(n_mix, n_all):
                own_weight(q).wait()

        @pl.when(keep)
        def _():
            for q in range(n_mix, n_all):
                wait_weight(q, i)

        owner = owner_of(i)
        term = lax.dot_general(
            hidden[...],
            wts[2, owner],
            (((1,), (1,)), ((), ())),
            preferred_element_type=jnp.float32,
        ).astype(jnp.bfloat16)

        @pl.when(mine(owner))
        def _():
            orecv[out_slot(owner)] = term

        @pl.when(jnp.logical_not(mine(owner)))
        def _():
            osend[i] = term
            out_copy(i, owner).start()

        return carry

    lax.fori_loop(0, 2, down_step, 0)
    on_lead((forward_z, ((5, far),)))
    lax.fori_loop(2, n_sp, down_step, 0)

    @pl.when(lead)
    def _():
        attq_copy(0).wait_recv()

    for s in range(orecv.shape[0]):

        @pl.when(lead | (s != source))
        @jax.named_scope("owait")
        def _():
            for half in range(parts):
                ref = orecv.at[s, :, pl.ds(half * depth, depth)]
                remote(ref, ref, out_s.at[0], out_r.at[s, half], sib).wait_recv()

    total = att_q[...].astype(jnp.float32)
    for s in range(orecv.shape[0]):
        total = total + orecv[s].astype(jnp.float32)
    result[...] = total.astype(jnp.bfloat16)
    store = pltpu.make_async_copy(result, output, local_sem.at[0])
    store.start()

    y_copy(0).wait_send()
    for i in (2, 3, 4):
        y_copy(i).wait_send()
    z_copy(1).wait_send()

    @pl.when(inner)
    def _():
        z_copy(3).wait_send()
        for i in (2, 3, 4):
            z_onward(i).wait_send()

    for i in range(1, n_sp):
        x_copy(i).wait_send()
        sib_copy(i).wait_send()
        xs_copy(i).wait_send()
    for d in range(n_tp - 1):
        gain_copy(d).wait_send()

    @pl.when(lead)
    def _():
        tap_copy().wait_send()
        for q in range(n_all):
            z_weight(q, 0, 2).wait_send()
            for k in (0, 2, 3, 4):
                y_weight(q, k).wait_send()
            for k in range(n_sp):
                sib_weight(q, k).wait_send()
        for t in range(n_steps):
            part_copy(t).wait_send()
            cross_copy(t).wait_send()

    @pl.when(keep)
    def _():
        attq_copy(0).wait_send()
        for q in range(n_all):
            z_weight(q, 0, 1).wait_send()
            z_weight(q, 1, 3).wait_send()
        for t in range(n_steps):
            bx_copy(t).wait_send()
            swap_copy(t).wait_send()

        @pl.when(sp > 0)
        def _():
            for plane in range(2):
                halo_copy(1, plane).wait_send()

        @pl.when(sp < n_sp - 1)
        def _():
            for plane in range(2):
                halo_copy(0, plane).wait_send()

    def out_wait(i, carry):
        owner = owner_of(i)

        @pl.when(jnp.logical_not(mine(owner)))
        def _():
            out_copy(i, owner).wait_send()

        return carry

    lax.fori_loop(0, n_sp, out_wait, 0)
    store.wait()


def fused_device(n_sp, n_tp, *arrays):
    (
        residual,
        query_wide,
        query_narrow,
        latent,
        rope_key,
        latent_gain,
        expand_wide,
        expand_narrow,
        out_wide,
        out_narrow,
        norm_gain,
        up_gate,
        up_value,
        down_weight,
        conv_taps,
    ) = arrays
    rows, features = residual.shape
    rank = latent.shape[1]
    depth, ff = up_gate.shape
    width = n_sp * depth
    fine, coarse = turn_tables(rows, n_sp)
    operands = (
        residual,
        query_wide,
        query_narrow,
        latent,
        rope_key.T,
        latent_gain[None],
        expand_wide,
        expand_narrow,
        out_wide,
        out_narrow,
        norm_gain[None],
        up_gate,
        up_value,
        down_weight,
        conv_taps,
        jnp.asarray(fine),
        jnp.asarray(coarse),
    )
    small = (5, 10, 14, 15, 16)
    anywhere = pl.BlockSpec(memory_space=pl.ANY)
    inside = pl.BlockSpec(memory_space=pltpu.VMEM)
    low, full = jnp.bfloat16, jnp.float32
    buffers = [
        ((n_sp, rows, rank + LANES), low),
        ((3, n_sp, depth, ff), low),
        ((rows, rank), low),
        ((ROPE, rows), low),
        (query_wide.shape, low),
        (query_narrow.shape, low),
        ((2, rows, 2 * LANES), low),
        ((2, rows, LANES), low),
        ((2, rows, 2 * LANES), low),
        ((2, rows, 2 * LANES), low),
        ((2, rows, LANES), low),
        ((2, rows, LANES), low),
        ((2, rows, 2 * LANES), full),
        ((2, rows, LANES), full),
        ((4, rows, LANES), full),
        ((rank, expand_wide.shape[1] + expand_narrow.shape[1]), low),
        ((out_wide.shape[0] + out_narrow.shape[0], width), low),
        ((rows, features), low),
        ((rows, out_wide.shape[0] + out_narrow.shape[0]), low),
        ((rows, width), low),
        ((rows, width), low),
        ((rows, width), low),
        ((rows, width), low),
        ((rows, features), low),
        ((rows + HALO, width), low),
        ((2, HALO, width), low),
        ((n_tp, 1, features), full),
        (conv_taps.shape, full),
        ((rows, ff), low),
        ((n_sp, rows, depth), low),
        ((4, rows, features), low),
        ((rows, features), low),
    ]
    steps = rows // LANES
    semaphores = [
        (9,),
        (8,),
        (8,),
        (8,),
        (8,),
        (4,),
        (5,),
        (5,),
        (8,),
        (8,),
        (8,),
        (6, 8),
        (6, 2),
        (6, 5),
        (6, 8),
        (steps,),
        (steps,),
        (steps,),
        (steps,),
        (steps,),
        (steps,),
        (steps,),
        (steps,),
        (2,),
        (2, 2),
        (1,),
        (1,),
        (3,),
        (3,),
        (1,),
        (1,),
        (4, features // depth),
        (8,),
    ]
    return pl.pallas_call(
        fused_kernel,
        out_shape=jax.ShapeDtypeStruct((rows, features), jnp.bfloat16),
        in_specs=[inside if i in small else anywhere for i in range(len(operands))],
        out_specs=anywhere,
        scratch_shapes=[pltpu.VMEM(shape, dtype) for shape, dtype in buffers]
        + [pltpu.SemaphoreType.DMA(shape) for shape in semaphores],
        compiler_params=pltpu.CompilerParams(
            collective_id=0, has_side_effects=True, vmem_limit_bytes=67043328
        ),
    )(*operands)


def solution(mesh):
    in_specs = (
        P("sp", "tp"),
        P("sp", "tp"),
        P("sp", "tp"),
        P("sp", None),
        P("sp", None),
        P(),
        P(None, "tp"),
        P(None, "tp"),
        P("tp", None),
        P("tp", None),
        P("tp"),
        P("sp", "tp"),
        P("sp", "tp"),
        P("sp", "tp"),
        P(None, None, "tp"),
    )
    out_specs = P("sp", "tp")
    n_sp, n_tp = mesh.shape["sp"], mesh.shape["tp"]
    body = per_device
    if (n_sp, n_tp) == (8, 4):
        body = functools.partial(fused_device, n_sp, n_tp)
    return jax.shard_map(
        body, mesh=mesh, in_specs=in_specs, out_specs=out_specs, check_vma=False
    )
```
